32 devices in a mesh: sp: 8 (over z, x), tp: 4 (over y, core).
Axes of the slice: x: 2, y: 2, z: 4, core: 2. Of those that a mesh axis runs over, the one named last changes fastest.
Arguments:
- residual_layer_input: bfloat16 [2048, 2048], P(('sp', 'tp')), may hold values from -6 to 6
- value_projected: bfloat16 [2048, 4096], P('sp', 'tp'), may hold values from -6 to 6
- key_projected: bfloat16 [2048, 2048], P('sp', 'tp'), may hold values from -6 to 6
- query_projected: bfloat16 [2048, 2048], P('sp', 'tp'), may hold values from -6 to 6
- output_gate_projected: bfloat16 [2048, 4096], P('sp', 'tp'), may hold values from -6 to 6
- step_projected_raw: bfloat16 [2, 2048, 64], P(None, 'sp', 'tp'), may hold values from -5.5 to 5
- head_decay_logarithm: float32 [2, 64], P(None, 'tp'), may hold values from -15 to -2.9
- position_extra_decay: float32 [2048, 64], P('sp', 'tp'), may hold values from -2.1 to 0
- value_filter_weight: bfloat16 [5, 4096], P(None, 'tp'), may hold values from -2.5 to 2.5
- key_filter_weight: bfloat16 [5, 2048], P(None, 'tp'), may hold values from -2.5 to 2.5
- query_filter_weight: bfloat16 [5, 2048], P(None, 'tp'), may hold values from -2.5 to 2.5
- head_norm_gain: float32 [4096], P('tp'), may hold values from 0.1 to 1.9
- mixer_output_matrix: bfloat16 [4096, 2048], P(None, 'tp'), may hold values from -0.09375 to 0.09375
- expert_norm_gain: float32 [2048], replicated, may hold values from 0.1 to 1.9
- routes: int32 [2048, 2], P('sp'), may hold values from 0 to 7, all different within a row; in each aligned block of 64 rows (0 to 63, 64 to 127, ...) at most 32 rows name the same one
- chosen_expert_weight: float32 [2048, 2], P(('sp', 'tp')), may hold values from 0.1 to 1
- expert_gate_matrix: bfloat16 [8, 2048, 4096], P('sp', None, 'tp'), may hold values from -0.125 to 0.125
- expert_up_matrix: bfloat16 [8, 2048, 4096], P('sp', None, 'tp'), may hold values from -0.125 to 0.125
- expert_down_matrix: bfloat16 [8, 4096, 2048], P('sp', 'tp'), may hold values from -0.09375 to 0.09375
Outputs:
- layer_output: bfloat16 [2048, 2048], P(('sp', 'tp'))
The draws below stay inside these ranges and needn't reach their ends.
Inputs may be any that keep to these rules, and one draw needn't show every extreme that they name: `routes`: each row names 2 different experts; the rows of one device (aligned blocks of 64 rows) name one expert 32 times at most, and that most is reached.
All inputs are finite; a program needn't handle non-finite values.
Results may differ from the reference program's by a relative error of at most 0.015.
Values may be sent and summed in bfloat16 or wider, within the bound.
A program may use at most 64 MiB of HBM per device.

```python
import math
import jax
import jax.numpy as jnp
import numpy as np
from jax import lax

D = 2048
HEAD_DIM = 64
HEADS = 64
INNER = 4096
GROUPS = 16
STATE = 128
BLOCK = 128
TAPS = 5
EXPERT_FF = 4096
TOP = 2
TOK_DEV = 256
TOKENS = 2048
ROWS_DEV = 64
EXPERTS = 8
CAPACITY = 32
FF_SHARE = 1024
N_TP = 4


def draw_step_projected_raw(key, part):
    noise_key, level_key = jax.random.split(key)
    noise_part = jnp.clip(jax.random.normal(noise_key, (2, TOKENS, HEADS), jnp.float32), -4.0, 4.0)
    segments = TOKENS // TOK_DEV
    first_key, second_key = jax.random.split(level_key)
    ranks = jnp.stack([jax.random.permutation(first_key, segments), jax.random.permutation(second_key, segments)]).astype(jnp.float32)
    shift = -1.5 + 2.5 * ranks / max(segments - 1, 1)
    shift_rows = jnp.repeat(shift, TOK_DEV, axis=1)
    return (noise_part + shift_rows[:, :, None]).astype(jnp.bfloat16)


def draw_head_decay_logarithm(key, part):
    pick_key, fast_key, slow_key = jax.random.split(key, 3)
    fast_share = 0.5
    fast_heads = jax.random.uniform(pick_key, (2, HEADS), jnp.float32) < fast_share
    fast_rate = jnp.exp(jax.random.uniform(fast_key, (2, HEADS), jnp.float32, math.log(1.0 / 60.0), math.log(1.0 / 20.0)))
    slow_rate = jax.random.uniform(slow_key, (2, HEADS), jnp.float32, 0.05, 0.6) / TOKENS
    return jnp.log(jnp.where(fast_heads, fast_rate, slow_rate)).astype(jnp.float32)


def draw_position_extra_decay(key, part):
    place_key, depth_key = jax.random.split(key)
    spots = jax.random.randint(place_key, (3,), 0, TOKENS)
    depth = jnp.log(jax.random.uniform(depth_key, (3, HEADS), jnp.float32, 0.5, 0.8))
    matches = (lax.broadcasted_iota(jnp.int32, (TOKENS, 3), 0) == spots[None, :]).astype(jnp.float32)
    return jnp.dot(matches, depth, precision=lax.Precision.HIGHEST).astype(jnp.float32)


def steps_of(rng, shape, cuts, smallest, high):
    loudness = 1.0
    for dim, parts in cuts:
        draws = jax.random.uniform(jax.random.fold_in(jax.random.fold_in(rng, 6), dim), (parts,), jnp.float32, smallest / len(cuts), high / len(cuts))
        loudness = loudness * jnp.repeat(jnp.exp(draws), shape[dim] // parts).reshape((-1,) + (1,) * (len(shape) - 1 - dim))
    return loudness


def routed_block(stream_key, own, number, rows, number_of, top, bound, skew):
    sequence = jax.random.permutation(stream_key, number_of)
    crowded, common = shares(number_of, rows * top, bound, skew, True), shares(number_of, rows * top, bound, skew, False)
    places = jnp.arange(number_of)

    def named(tallies, rotation):
        used = int((tallies > 0).sum())
        fixed = max(1, used // 4)
        moved = fixed + (places - fixed + rotation * (used - fixed)) % max(1, number_of - fixed)
        return jnp.zeros((number_of,), jnp.int32).at[sequence[jnp.where(places < fixed, places, moved)]].set(jnp.asarray(tallies, jnp.int32))

    tallies = jnp.where(number % 4 == 0, named(crowded, number // 4), named(common, number - number // 4 - 1))
    mixed = jax.random.permutation(jax.random.fold_in(own, 3), number_of)
    giver, taker = mixed[0:number_of // 2 * 2:2], mixed[1:number_of // 2 * 2:2]
    room = jnp.minimum(tallies[giver] - 1, bound - tallies[taker]) // 2
    room = jnp.where((giver == sequence[0]) | (taker == sequence[0]) | (tallies[taker] == 0), 0, jnp.maximum(room, 0))
    moved = jax.random.randint(jax.random.fold_in(own, 4), (number_of // 2,), 0, 1 << 20) % (room + 1)
    tallies = tallies.at[giver].add(-moved).at[taker].add(moved)
    labels = jnp.searchsorted(jnp.cumsum(tallies), jnp.arange(rows * top), side="right").astype(jnp.int32)
    grid = labels.reshape(top, rows).T
    grid = grid[jax.random.permutation(jax.random.fold_in(own, 1), rows)]
    rotation = jax.random.randint(jax.random.fold_in(own, 2), (rows, 1), 0, top)
    return jnp.take_along_axis(grid, (jnp.arange(top)[None, :] + rotation) % top, axis=1)


def shares(count, total, reach, lean, full):
    loads = [(1 << 20) // math.isqrt(rank ** lean) + 1 for rank in range(1, count + 1)]
    largest = reach if full else min(reach, max(-(-total // count), total * loads[0] // sum(loads)))
    least = 1 if total - largest >= count - 1 else 0
    counts, surplus = [largest] + [least] * (count - 1), total - largest - least * (count - 1)
    while surplus > 0:
        candidates = [i for i in range(1, count) if counts[i] < largest] or [i for i in range(1, count) if counts[i] < reach]
        whole, remaining = sum([loads[i] for i in candidates]), surplus
        for i in candidates:
            extra = min(reach - counts[i], max(1, remaining * loads[i] // whole), surplus)
            counts[i] = counts[i] + extra
            surplus = surplus - extra
    return np.array(counts)


def gaussian(stream_key, dims, scale, reach, shards=(), held_as=jnp.bfloat16):
    values = scale * jax.random.normal(stream_key, dims, jnp.float32)
    if shards:
        values = values * steps_of(stream_key, dims, shards, -0.22, 0.18)
    return jnp.clip(values, -reach, reach).astype(held_as)


def setup_inputs(seed: int = 0) -> dict:
    arg_keys = jax.random.split(jax.random.key(seed), 20)
    residual_layer_input = gaussian(arg_keys[0], (TOKENS, D), 1.0, 6.0, ((0, 32),))
    value_projected = gaussian(arg_keys[1], (TOKENS, INNER), 1.0, 6.0, ((0, 8), (1, 4)))
    key_projected = gaussian(arg_keys[2], (TOKENS, GROUPS * STATE), 1.0, 6.0, ((0, 8), (1, 4)))
    query_projected = gaussian(arg_keys[3], (TOKENS, GROUPS * STATE), 1.0, 6.0, ((0, 8), (1, 4)))
    output_gate_projected = gaussian(arg_keys[4], (TOKENS, INNER), 1.0, 6.0, ((0, 8), (1, 4)))
    step_projected_raw = draw_step_projected_raw(jax.random.fold_in(arg_keys[19], 71), 0)
    head_decay_logarithm = draw_head_decay_logarithm(jax.random.fold_in(arg_keys[19], 71), 0)
    position_extra_decay = draw_position_extra_decay(jax.random.fold_in(arg_keys[19], 71), 0)
    value_filter_weight = gaussian(arg_keys[8], (TAPS, INNER), TAPS ** -0.5, 2.5, ((1, 4),))
    key_filter_weight = gaussian(arg_keys[9], (TAPS, GROUPS * STATE), TAPS ** -0.5, 2.5, ((1, 4),))
    query_filter_weight = gaussian(arg_keys[10], (TAPS, GROUPS * STATE), TAPS ** -0.5, 2.5, ((1, 4),))
    head_norm_gain = jnp.clip(1.0 + 0.18 * jax.random.normal(arg_keys[11], (INNER,), jnp.float32), 0.1, 1.9)
    mixer_output_matrix = gaussian(arg_keys[12], (INNER, D), INNER ** -0.5, 0.09375, ((1, 4),))
    expert_norm_gain = jnp.clip(1.0 + 0.18 * jax.random.normal(arg_keys[13], (D,), jnp.float32), 0.1, 1.9)
    routes_keys = jax.random.split(jax.random.fold_in(arg_keys[14], 1), TOKENS // ROWS_DEV)
    routes_turns = jax.random.permutation(jax.random.fold_in(arg_keys[14], 3), TOKENS // ROWS_DEV)
    routes = jax.vmap(lambda own, number: routed_block(jax.random.fold_in(arg_keys[14], 2), own, number, ROWS_DEV, EXPERTS, TOP, CAPACITY, 1))(routes_keys, routes_turns).reshape((TOKENS, TOP))
    chosen_expert_weight = jnp.clip(0.1 + 0.9 * jax.random.uniform(arg_keys[15], (TOKENS, TOP), jnp.float32) ** steps_of(arg_keys[15], (TOKENS, TOP), ((0, 32),), -0.2, 0.2), 0.1, 1.0)
    expert_gate_matrix = gaussian(arg_keys[16], (EXPERTS, D, EXPERT_FF), D ** -0.5, 0.125, ((0, 8), (2, 4)))
    expert_up_matrix = gaussian(arg_keys[17], (EXPERTS, D, EXPERT_FF), D ** -0.5, 0.125, ((0, 8), (2, 4)))
    expert_down_matrix = gaussian(arg_keys[18], (EXPERTS, EXPERT_FF, D), EXPERT_FF ** -0.5, 0.09375, ((0, 8), (1, 4)))
    return {"residual_layer_input": residual_layer_input, "value_projected": value_projected, "key_projected": key_projected, "query_projected": query_projected, "output_gate_projected": output_gate_projected, "step_projected_raw": step_projected_raw, "head_decay_logarithm": head_decay_logarithm, "position_extra_decay": position_extra_decay, "value_filter_weight": value_filter_weight, "key_filter_weight": key_filter_weight, "query_filter_weight": query_filter_weight, "head_norm_gain": head_norm_gain, "mixer_output_matrix": mixer_output_matrix, "expert_norm_gain": expert_norm_gain, "routes": routes, "chosen_expert_weight": chosen_expert_weight, "expert_gate_matrix": expert_gate_matrix, "expert_up_matrix": expert_up_matrix, "expert_down_matrix": expert_down_matrix}


epsilon = 1e-06

def centred_taps(inputs, taps):
    length = inputs.shape[0]
    half_width = (taps.shape[0] - 1) // 2
    padded = jnp.pad(inputs.astype(jnp.float32), ((half_width, half_width), (0, 0)))
    weights = taps.astype(jnp.float32)
    result = weights[0] * padded[0:length]
    for offset in range(1, taps.shape[0]):
        result = result + weights[offset] * padded[offset:offset + length]
    return result

def block_terms(operands):
    forward_cum, backward_excl, forward_part, backward_part, key_rows, query_rows = operands
    scores = jnp.einsum('lgn,sgn->lsg', query_rows.astype(jnp.float32), key_rows.astype(jnp.float32))
    position = jnp.arange(scores.shape[0], dtype=jnp.int32)
    lower_mask = (position[None, :] <= position[:, None])[:, :, None, None]
    upper_mask = (position[None, :] >= position[:, None])[:, :, None, None]
    forward_gap = jnp.where(lower_mask, forward_cum[:, None] - forward_cum[None, :], -jnp.inf)
    backward_gap = jnp.where(upper_mask, backward_excl[None, :] - backward_excl[:, None], -jnp.inf)
    forward_weight = (scores[..., None] * jnp.exp(forward_gap)).astype(jnp.bfloat16)
    backward_weight = (scores[..., None] * jnp.exp(backward_gap)).astype(jnp.bfloat16)
    inner = jnp.einsum('lsgh,sghp->lghp', forward_weight.astype(jnp.float32), forward_part.astype(jnp.float32))
    inner = inner + jnp.einsum('lsgh,sghp->lghp', backward_weight.astype(jnp.float32), backward_part.astype(jnp.float32))
    key_wide = key_rows.astype(jnp.float32)[:, :, None, :]
    forward_keys = (jnp.exp(forward_cum[-1][None] - forward_cum)[..., None] * key_wide).astype(jnp.bfloat16)
    backward_keys = (jnp.exp(backward_excl)[..., None] * key_wide).astype(jnp.bfloat16)
    forward_state = jnp.einsum('sghn,sghp->ghpn', forward_keys.astype(jnp.float32), forward_part.astype(jnp.float32))
    backward_state = jnp.einsum('sghn,sghp->ghpn', backward_keys.astype(jnp.float32), backward_part.astype(jnp.float32))
    return (inner, forward_state, backward_state)

def advance(carried, operands):
    block_state, block_total = operands
    return (jnp.exp(block_total)[..., None, None] * carried + block_state, carried)

def apply_expert(operands):
    slot_block, gate_part, up_part, down_part = operands
    gate_value = jnp.dot(slot_block, gate_part, preferred_element_type=jnp.float32)
    up_value = jnp.dot(slot_block, up_part, preferred_element_type=jnp.float32)
    hidden = (jax.nn.silu(gate_value) * up_value).astype(jnp.bfloat16)
    pieces = jnp.einsum('rjf,jfd->jrd', hidden.reshape(slot_block.shape[0], N_TP, FF_SHARE).astype(jnp.float32), down_part.reshape(N_TP, FF_SHARE, D).astype(jnp.float32)).astype(jnp.bfloat16)
    return lax.optimization_barrier(jnp.sum(pieces.astype(jnp.float32), axis=0)).astype(jnp.bfloat16)

def reference(residual_layer_input, value_projected, key_projected, query_projected, output_gate_projected, step_projected_raw, head_decay_logarithm, position_extra_decay, value_filter_weight, key_filter_weight, query_filter_weight, head_norm_gain, mixer_output_matrix, expert_norm_gain, routes, chosen_expert_weight, expert_gate_matrix, expert_up_matrix, expert_down_matrix):
    tokens = value_projected.shape[0]
    per_group = HEADS // GROUPS
    blocks = tokens // BLOCK
    values = centred_taps(value_projected, value_filter_weight).astype(jnp.bfloat16)
    key_rows = jax.nn.silu(centred_taps(key_projected, key_filter_weight)).astype(jnp.bfloat16).reshape(blocks, BLOCK, GROUPS, STATE)
    query_rows = jax.nn.silu(centred_taps(query_projected, query_filter_weight)).astype(jnp.bfloat16).reshape(blocks, BLOCK, GROUPS, STATE)
    positive_step_sizes = jax.nn.softplus(step_projected_raw.astype(jnp.float32))
    decay_logarithm = -jnp.exp(head_decay_logarithm)[:, None, :] * positive_step_sizes + position_extra_decay[None]
    scaled = (values.astype(jnp.float32).reshape(tokens, HEADS, HEAD_DIM)[None] * positive_step_sizes[..., None]).astype(jnp.bfloat16)
    scaled = scaled.reshape(2, blocks, BLOCK, GROUPS, per_group, HEAD_DIM)
    log_blocks = decay_logarithm.reshape(2, blocks, BLOCK, GROUPS, per_group)
    running = jnp.cumsum(log_blocks, axis=2)
    forward_cum = running[0]
    backward_excl = running[1] - log_blocks[1]
    forward_total = running[0][:, -1]
    backward_total = running[1][:, -1]
    inner, forward_state, backward_state = lax.map(block_terms, (forward_cum, backward_excl, scaled[0], scaled[1], key_rows, query_rows))
    zero_state = jnp.zeros((GROUPS, per_group, HEAD_DIM, STATE), jnp.float32)
    entering = lax.scan(advance, zero_state, (forward_state, forward_total))[1]
    leaving = lax.scan(advance, zero_state, (backward_state, backward_total), reverse=True)[1]
    query_wide = query_rows.astype(jnp.float32)
    forward_read = jnp.exp(forward_cum)[..., None] * jnp.einsum('blgn,bghpn->blghp', query_wide, entering.astype(jnp.bfloat16).astype(jnp.float32))
    backward_read = jnp.exp(backward_total[:, None] - backward_excl)[..., None] * jnp.einsum('blgn,bghpn->blghp', query_wide, leaving.astype(jnp.bfloat16).astype(jnp.float32))
    mixer_raw = (inner + forward_read + backward_read).reshape(tokens, HEADS, HEAD_DIM)
    gated = mixer_raw * jax.nn.silu(output_gate_projected.astype(jnp.float32)).reshape(tokens, HEADS, HEAD_DIM)
    inverse_rms = lax.rsqrt(lax.optimization_barrier(jnp.mean(gated * gated, axis=-1, keepdims=True)) + epsilon)
    head_normed = (gated * inverse_rms * head_norm_gain.reshape(HEADS, HEAD_DIM)).astype(jnp.bfloat16)
    head_normed = head_normed.reshape(tokens, HEADS * HEAD_DIM)
    mixer_out = jnp.dot(head_normed, mixer_output_matrix, preferred_element_type=jnp.float32).astype(jnp.bfloat16)
    middle = (residual_layer_input.astype(jnp.float32) + mixer_out.astype(jnp.float32)).astype(jnp.bfloat16)
    residual = middle.astype(jnp.float32)
    normed = (residual * lax.rsqrt(lax.optimization_barrier(jnp.mean(residual * residual, axis=-1, keepdims=True)) + epsilon) * expert_norm_gain).astype(jnp.bfloat16)
    device_blocks = tokens // ROWS_DEV
    slots_each = device_blocks * CAPACITY
    flat_routes = routes.reshape(device_blocks, ROWS_DEV * TOP).astype(jnp.int32)
    matches = (flat_routes[:, :, None] == jnp.arange(EXPERTS, dtype=jnp.int32)[None, None, :]).astype(jnp.int32)
    earlier = (jnp.cumsum(matches, axis=1) - matches).astype(jnp.int32)
    rank_in = lax.optimization_barrier(jnp.sum(matches * earlier, axis=2)).astype(jnp.int32)
    block_index = jnp.arange(device_blocks, dtype=jnp.int32)[:, None]
    slot_ids = (flat_routes * slots_each + block_index * CAPACITY + rank_in).reshape(-1).astype(jnp.int32)
    copies = jnp.repeat(normed, TOP, axis=0)
    slot_rows = jnp.zeros((EXPERTS * slots_each, D), jnp.bfloat16).at[slot_ids].set(copies)
    expert_out = lax.map(apply_expert, (slot_rows.reshape(EXPERTS, slots_each, D), expert_gate_matrix, expert_up_matrix, expert_down_matrix))
    picked = expert_out.reshape(EXPERTS * slots_each, D)[slot_ids].astype(jnp.float32).reshape(tokens, TOP, D)
    expert_mix = lax.optimization_barrier(jnp.sum(picked * chosen_expert_weight[:, :, None], axis=1))
    return (residual + expert_mix).astype(jnp.bfloat16)
```

```python
import functools

import jax
import jax.numpy as jnp
from jax import lax
from jax.experimental import pallas as pl
from jax.experimental.pallas import tpu as pltpu
from jax.sharding import PartitionSpec as P

HEAD_DIM = 64
STATE = 128
BLOCK = 128
TAPS = 5


epsilon = 1e-06
highest = lax.Precision.HIGHEST


MESH = pl.DeviceIdType.MESH


def remote(src, dst, send, recv, device):
    return pltpu.make_async_remote_copy(
        src_ref=src,
        dst_ref=dst,
        send_sem=send,
        recv_sem=recv,
        device_id=device,
        device_id_type=MESH,
    )


def greet(devices):
    barrier = pltpu.get_barrier_semaphore()
    for device in devices:
        pl.semaphore_signal(barrier, inc=1, device_id=device, device_id_type=MESH)
    pl.semaphore_wait(barrier, len(devices))


def vmem(count):
    return [pl.BlockSpec(memory_space=pltpu.VMEM)] * count


def dma(*shape):
    return pltpu.SemaphoreType.DMA(shape)


def params(number):
    return pltpu.CompilerParams(collective_id=number, has_side_effects=True)


def each(count, body):
    lax.fori_loop(0, count, lambda k, _: (body(k), 0)[1], 0)


def exchange_kernel(axis, n, k, *refs):
    ins, outs = refs[:k], refs[k : 2 * k]
    send, recv, local = refs[2 * k :]
    me = lax.axis_index(axis)
    greet([{axis: lax.rem(me + d, n)} for d in range(1, n)])
    copies = []
    for d in range(1, n):
        peer = lax.rem(me + d, n)
        for a in range(k):
            copies.append(
                remote(ins[a].at[peer], outs[a].at[me], send.at[a, d], recv.at[a, d], {axis: peer})
            )
    for a in range(k):
        copies.append(pltpu.make_async_copy(ins[a].at[me], outs[a].at[me], local.at[a]))
    for copy in copies:
        copy.start()
    for copy in copies:
        copy.wait()


def exchange(arrays, axis, number):
    n, k = lax.axis_size(axis), len(arrays)
    return pl.pallas_call(
        functools.partial(exchange_kernel, axis, n, k),
        out_shape=[jax.ShapeDtypeStruct(a.shape, a.dtype) for a in arrays],
        in_specs=vmem(k),
        out_specs=vmem(k),
        scratch_shapes=[dma(k, n), dma(k, n), dma(k)],
        compiler_params=params(number),
    )(*arrays)


def edges_kernel(n, x, out, send, recv):
    me = lax.axis_index("sp")
    left, right = lax.rem(me + n - 1, n), lax.rem(me + 1, n)
    greet([{"sp": left}, {"sp": right}])
    copies = [
        remote(x.at[1], out.at[0], send.at[0], recv.at[0], {"sp": right}),
        remote(x.at[0], out.at[1], send.at[1], recv.at[1], {"sp": left}),
    ]
    for copy in copies:
        copy.start()
    for copy in copies:
        copy.wait()


def edges(x, number):
    return pl.pallas_call(
        functools.partial(edges_kernel, lax.axis_size("sp")),
        out_shape=jax.ShapeDtypeStruct(x.shape, x.dtype),
        in_specs=vmem(1),
        out_specs=vmem(1)[0],
        scratch_shapes=[dma(2), dma(2)],
        compiler_params=params(number),
    )(x)


def tp_places(tp):
    j = lax.axis_index("tp")
    core = lax.rem(j, 2)
    chip = lax.div(j, 2)
    return j, chip, core, tp // 2, chip * 2 + (1 - core)


def gather_kernel(tp, pieces, x, out, send, recv, rsend, rrecv, local):
    j, chip, core, chips, partner = tp_places(tp)
    width = x.shape[1]
    piece = x.shape[0] // pieces
    others = [lax.rem(chip + d, chips) * 2 + core for d in range(1, chips)]
    greet([{"tp": o} for o in others] + [{"tp": partner}])

    def place(b, r):
        return out.at[pl.ds(r * piece, piece), pl.ds(pl.multiple_of(b * width, 128), width)]

    own = pltpu.make_async_copy(
        x, out.at[:, pl.ds(pl.multiple_of(j * width, 128), width)], local.at[0]
    )
    own.start()
    waits = []
    for r in range(pieces):
        part = x.at[pl.ds(r * piece, piece)]
        for d in range(1, chips):
            copy = remote(part, place(j, r), send.at[r, d], recv.at[r, d], {"tp": others[d - 1]})
            copy.start()
            waits.append(copy)
    relays = []
    for r in range(pieces):
        part = x.at[pl.ds(r * piece, piece)]
        copy = remote(part, place(j, r), rsend.at[r, 0], rrecv.at[r, 0], {"tp": partner})
        copy.start()
        relays.append(copy)
    for r in range(pieces):
        for d in range(1, chips):
            came = lax.rem(chip + chips - d, chips) * 2 + core
            spot = place(came, r)
            remote(spot, spot, send.at[r, d], recv.at[r, d], {"tp": partner}).wait_recv()
            copy = remote(spot, spot, rsend.at[r, d], rrecv.at[r, d], {"tp": partner})
            copy.start()
            relays.append(copy)
    for copy in waits:
        copy.wait_send()
    for copy in relays:
        copy.wait()
    own.wait()


def gather_columns(x, number, pieces=2):
    tp = lax.axis_size("tp")
    sems = dma(pieces, tp // 2)
    return pl.pallas_call(
        functools.partial(gather_kernel, tp, pieces),
        out_shape=jax.ShapeDtypeStruct((x.shape[0], x.shape[1] * tp), x.dtype),
        in_specs=vmem(1),
        out_specs=vmem(1)[0],
        scratch_shapes=[sems, sems, sems, sems, dma(1)],
        compiler_params=params(number),
    )(x)


def spread_kernel(sp, tp, ahead, x, out, asend, arecv, fsend, frecv, rsend, rrecv, local):
    me = lax.axis_index("sp")
    j, chip, core, chips, partner = tp_places(tp)
    others = [lax.rem(chip + d, chips) * 2 + core for d in range(1, chips)]
    greet(
        [{"sp": lax.rem(me + d, sp)} for d in range(1, sp)]
        + [{"tp": o} for o in others]
        + [{"tp": partner}]
    )

    def across(d):
        peer = lax.rem(me + d, sp)
        return remote(x.at[peer], out.at[j, me], asend.at[d], arecv.at[d], {"sp": peer})

    def forward(d, k):
        spot = out.at[j, lax.rem(me + sp - d, sp)]
        return remote(spot, spot, fsend.at[d, k], frecv.at[d, k], {"tp": others[k - 1]})

    def relay(d, k):
        came = lax.rem(chip + chips - k, chips) * 2 + core
        spot = out.at[came, lax.rem(me + sp - d, sp)]
        return remote(spot, spot, rsend.at[d, k], rrecv.at[d, k], {"tp": partner})

    own = pltpu.make_async_copy(x.at[me], out.at[j, me], local.at[0])
    own.start()
    each(min(ahead, sp - 1), lambda d: across(d + 1).start())

    def onward(d):
        for k in range(1, chips):
            forward(d, k).start()
        relay(d, 0).start()

    def pass_on(d):
        for k in range(1, chips):
            forward(d, k).wait_recv()
            relay(d, k).start()

    own.wait()
    onward(0)

    def step(d):
        across(d + 1).wait_recv()

        @pl.when(d + 1 + ahead < sp)
        def _():
            across(d + 1 + ahead).start()

        onward(d + 1)
        pass_on(d)

    each(sp - 1, step)
    pass_on(sp - 1)

    def finish(d):
        for k in range(1, chips):
            forward(d, k).wait_send()
        for k in range(chips):
            relay(d, k).wait()

    each(sp, finish)
    each(sp - 1, lambda d: across(d + 1).wait_send())


def spread_rows(x, number):
    sp, tp = lax.axis_size("sp"), lax.axis_size("tp")
    pair = dma(sp, tp // 2)
    return pl.pallas_call(
        functools.partial(spread_kernel, sp, tp, 3),
        out_shape=jax.ShapeDtypeStruct((tp,) + x.shape, x.dtype),
        in_specs=vmem(1),
        out_specs=vmem(1)[0],
        scratch_shapes=[dma(sp), dma(sp), pair, pair, pair, pair, dma(1)],
        compiler_params=params(number),
    )(x)


def collect_kernel(
    sp, tp, x, out, first, joined, second, total, csend, crecv, fsend, frecv, asend, arecv, local
):
    me = lax.axis_index("sp")
    j, chip, core, chips, partner = tp_places(tp)
    others = [lax.rem(chip + d, chips) * 2 + core for d in range(1, chips)]
    greet(
        [{"sp": lax.rem(me + d, sp)} for d in range(1, sp)]
        + [{"tp": o} for o in others]
        + [{"tp": partner}]
    )

    def rows(d):
        return lax.rem(me + d, sp)

    def aim(k):
        return lax.rem(chip + k, chips)

    def beside(d, k):
        s = rows(d)
        return remote(
            x.at[aim(k) * 2 + (1 - core), s],
            first.at[k, s],
            csend.at[d, k],
            crecv.at[d, k],
            {"tp": partner},
        )

    def over(d, k):
        s = rows(d)
        return remote(
            joined.at[k, s], second.at[k, s], fsend.at[d, k], frecv.at[d, k], {"tp": others[k - 1]}
        )

    def back(d):
        s = rows(d)
        return remote(total.at[s], out.at[me], asend.at[d], arecv.at[d], {"sp": s})

    def begin(i):
        d = lax.rem(i + 1, sp)
        for k in range(chips):
            beside(d, lax.rem(k + 1, chips)).start()

    each(sp, begin)

    def join(d):
        s = rows(d)
        for k in range(1, chips):
            beside(d, k).wait_recv()
            mine = x[aim(k) * 2 + core, s].astype(jnp.float32)
            joined[k, s] = (mine + first[k, s].astype(jnp.float32)).astype(joined.dtype)
            over(d, k).start()

    def close(d):
        s = rows(d)
        beside(d, 0).wait_recv()
        value = x[j, s].astype(jnp.float32) + first[0, s].astype(jnp.float32)
        for k in range(1, chips):
            over(d, k).wait_recv()
            value = value + second[k, s].astype(jnp.float32)
        total[s] = value.astype(total.dtype)

    join(lax.rem(1, sp))

    def step(i):
        join(lax.rem(i + 2, sp))
        close(i + 1)
        back(i + 1).start()

    each(sp - 1, step)
    close(0)
    own = pltpu.make_async_copy(total.at[me], out.at[me], local.at[0])
    own.start()

    def finish(d):
        for k in range(chips):
            beside(d, k).wait_send()
        for k in range(1, chips):
            over(d, k).wait_send()

    each(sp, finish)
    each(sp - 1, lambda d: back(d + 1).wait())
    own.wait()


def collect_rows(x, number):
    sp, tp = lax.axis_size("sp"), lax.axis_size("tp")
    chips = tp // 2
    pair = dma(sp, chips)
    buffer = pltpu.VMEM((chips,) + x.shape[1:], x.dtype)
    return pl.pallas_call(
        functools.partial(collect_kernel, sp, tp),
        out_shape=jax.ShapeDtypeStruct(x.shape[1:], x.dtype),
        in_specs=vmem(1),
        out_specs=vmem(1)[0],
        scratch_shapes=[
            buffer,
            buffer,
            buffer,
            pltpu.VMEM(x.shape[1:], x.dtype),
            pair,
            pair,
            pair,
            pair,
            dma(sp),
            dma(sp),
            dma(1),
        ],
        compiler_params=params(number),
    )(x)


def flip(me, d):
    out, bit = me, 1
    while bit <= d:
        if d & bit:
            out = out + bit * (1 - 2 * lax.rem(lax.div(out, bit), 2))
        bit *= 2
    return out


def expert_kernel(
    sp, tp, x, wgate, wup, wdown, out,
    arr, part, hidden, first, joined, second, total, vgate, vup, vdown,
    asend, arecv, fsend, frecv, rsend, rrecv, csend, crecv, osend, orecv, bsend, brecv, local, load,
):
    me = lax.axis_index("sp")
    j, chip, core, chips, partner = tp_places(tp)
    others = [lax.rem(chip + d, chips) * 2 + core for d in range(1, chips)]
    cap, width = x.shape[1], x.shape[2]
    ff = vgate.shape[1]
    rows = 2 * tp * cap
    loads = [
        pltpu.make_async_copy(wgate.at[0], vgate, load.at[0]),
        pltpu.make_async_copy(wup.at[0], vup, load.at[1]),
        pltpu.make_async_copy(wdown.at[0], vdown, load.at[2]),
    ]
    for copy in loads:
        copy.start()
    own = pltpu.make_async_copy(x.at[me], arr.at[me, j], local.at[0])
    own.start()
    greet(
        [{"sp": flip(me, d)} for d in range(1, sp)]
        + [{"tp": o} for o in others]
        + [{"tp": partner}]
    )

    def across(d):
        peer = flip(me, d)
        return remote(x.at[peer], arr.at[me, j], asend.at[d], arecv.at[d], {"sp": peer})

    def forward(d, k):
        spot = arr.at[flip(me, d), j]
        return remote(spot, spot, fsend.at[d, k], frecv.at[d, k], {"tp": others[k - 1]})

    def relay(d, k):
        came = lax.rem(chip + chips - k, chips) * 2 + core
        spot = arr.at[flip(me, d), came]
        return remote(spot, spot, rsend.at[d, k], rrecv.at[d, k], {"tp": partner})

    def onward(d):
        if d == 0:
            own.wait()
        else:
            across(d).wait_recv()
        for k in range(1, chips):
            forward(d, k).start()
        relay(d, 0).start()

    def pass_on(d):
        for k in range(1, chips):
            forward(d, k).wait_recv()
            relay(d, k).start()

    def aim(k):
        return lax.rem(chip + k, chips)

    def beside(d, k):
        s = flip(me, d)
        return remote(
            part.at[s, aim(k) * 2 + (1 - core)],
            first.at[s, k],
            csend.at[d, k],
            crecv.at[d, k],
            {"tp": partner},
        )

    def over(d, k):
        s = flip(me, d)
        return remote(
            joined.at[s, k], second.at[s, k], osend.at[d, k], orecv.at[d, k], {"tp": others[k - 1]}
        )

    def back(d):
        s = flip(me, d)
        return remote(total.at[s], out.at[me], bsend.at[d], brecv.at[d], {"sp": s})

    def begin(d):
        for k in range(chips):
            beside(d, (k + 1) % chips).start()

    def join(d):
        s = flip(me, d)
        for k in range(1, chips):
            beside(d, k).wait_recv()
            mine = part[s, aim(k) * 2 + core].astype(jnp.float32)
            joined[s, k] = (mine + first[s, k].astype(jnp.float32)).astype(joined.dtype)
            over(d, k).start()

    def close(d):
        s = flip(me, d)
        beside(d, 0).wait_recv()
        value = part[s, j].astype(jnp.float32) + first[s, 0].astype(jnp.float32)
        for k in range(1, chips):
            over(d, k).wait_recv()
            value = value + second[s, k].astype(jnp.float32)
        if d == 0:
            out[me] = value.astype(out.dtype)
        else:
            total[s] = value.astype(total.dtype)
            back(d).start()

    tile = min(ff, 256)
    wide = min(width, 256)

    def gate_up(g):
        base = flip(me, 2 * g) - lax.rem(flip(me, 2 * g), 2)

        def step(f):
            cols = pl.ds(pl.multiple_of(f * tile, tile), tile)
            held = arr[pl.ds(base, 2)].reshape(rows, width)
            gate = jnp.dot(held, vgate[:, cols], preferred_element_type=jnp.float32)
            up = jnp.dot(held, vup[:, cols], preferred_element_type=jnp.float32)
            hidden[:, cols] = (gate / (1.0 + jnp.exp(-gate)) * up).astype(hidden.dtype)

        each(ff // tile, step)

    def down(g):
        base = flip(me, 2 * g) - lax.rem(flip(me, 2 * g), 2)

        def step(f):
            cols = pl.ds(pl.multiple_of(f * wide, wide), wide)
            value = jnp.dot(hidden[...], vdown[:, cols], preferred_element_type=jnp.float32)
            part[pl.ds(base, 2), :, :, cols] = value.astype(part.dtype).reshape(2, tp, cap, wide)

        each(width // wide, step)

    for d in range(1, sp):
        across(d).start()
    ahead = min(4, sp)
    onward(0)
    onward(1)
    onward(2)
    pass_on(0)
    onward(3)
    pass_on(1)
    for copy in loads[:2]:
        copy.wait()
    for g in range(sp // 2):
        for d in (2 * g, 2 * g + 1):
            if g > 0:
                pass_on(d)
        for d in (2 * g, 2 * g + 1):
            for k in range(chips):
                relay(d, k).wait_recv()
        gate_up(g)
        for d in (2 * g + ahead, 2 * g + ahead + 1):
            if d < sp:
                onward(d)
        if g == 0:
            loads[2].wait()
        down(g)
        begin(2 * g)
        begin(2 * g + 1)
        if g > 0:
            close(2 * g - 2)
            close(2 * g - 1)
        join(2 * g)
        join(2 * g + 1)
    close(sp - 2)
    close(sp - 1)
    for d in range(sp):
        for k in range(1, chips):
            forward(d, k).wait_send()
            over(d, k).wait_send()
        for k in range(chips):
            relay(d, k).wait_send()
            beside(d, k).wait_send()
        if d > 0:
            across(d).wait_send()
            back(d).wait()


def run_experts(x, wgate, wup, wdown, number):
    sp, tp = lax.axis_size("sp"), lax.axis_size("tp")
    chips = tp // 2
    cap, width = x.shape[1:]
    ff = wgate.shape[2]
    kind = x.dtype
    pair = dma(sp, chips)
    line = dma(sp)
    piece = pltpu.VMEM((sp, chips, cap, width), kind)
    return pl.pallas_call(
        functools.partial(expert_kernel, sp, tp),
        out_shape=jax.ShapeDtypeStruct(x.shape, kind),
        in_specs=vmem(1) + [pl.BlockSpec(memory_space=pl.ANY)] * 3,
        out_specs=vmem(1)[0],
        scratch_shapes=[
            pltpu.VMEM((sp, tp, cap, width), kind),
            pltpu.VMEM((sp, tp, cap, width), kind),
            pltpu.VMEM((2 * tp * cap, ff), kind),
            piece,
            piece,
            piece,
            pltpu.VMEM((sp, cap, width), kind),
            pltpu.VMEM(wgate.shape[1:], kind),
            pltpu.VMEM(wup.shape[1:], kind),
            pltpu.VMEM(wdown.shape[1:], kind),
            line, line, pair, pair, pair, pair, pair, pair, pair, pair, line, line, dma(1), dma(3),
        ],
        compiler_params=pltpu.CompilerParams(
            collective_id=number, has_side_effects=True, vmem_limit_bytes=56 * 2**20
        ),
    )(x, wgate, wup, wdown)


def padded_2(cells, width):
    count, here = lax.axis_size("sp"), lax.axis_index("sp")
    came = edges(jnp.stack([cells[:width], cells[-width:]]), 1)
    before = jnp.where(here > 0, came[0], jnp.zeros_like(came[0]))
    after = jnp.where(here < count - 1, came[1], jnp.zeros_like(came[1]))
    return jnp.concatenate([before, cells, after], axis=0)


def carried_states(forward_sum, forward_final, backward_sum, backward_final):
    count = lax.axis_size("sp")
    shape = forward_final.shape
    per_head = shape[-2]
    states = jnp.stack([forward_final, backward_final]).astype(jnp.bfloat16)
    states = states.reshape(2, count, -1, shape[-1]).swapaxes(0, 1)
    totals = jnp.stack([forward_sum, backward_sum]).reshape(2, -1)
    totals = jnp.repeat(totals, per_head, axis=1).reshape(2, count, -1).swapaxes(0, 1)
    states, totals = exchange([states, totals], "sp", 2)
    factors = jnp.exp(totals)[..., None]
    parts = states.astype(jnp.float32)
    forward, backward = [], []
    held = jnp.zeros(parts.shape[2:], jnp.float32)
    for s in range(count):
        forward.append(held)
        held = factors[s, 0] * held + parts[s, 0]
    held = jnp.zeros(parts.shape[2:], jnp.float32)
    for s in reversed(range(count)):
        backward.append(held)
        held = factors[s, 1] * held + parts[s, 1]
    both = jnp.stack([jnp.stack(forward), jnp.stack(backward[::-1])], axis=1)
    (both,) = exchange([both.astype(jnp.bfloat16)], "sp", 3)
    both = both.astype(jnp.float32)
    return both[:, 0].reshape(shape), both[:, 1].reshape(shape)


def prefix_matrix(length):
    row_index = lax.broadcasted_iota(jnp.int32, (length, length), 0)
    column_index = lax.broadcasted_iota(jnp.int32, (length, length), 1)
    return (column_index <= row_index).astype(jnp.float32)


def local_chain(states, totals, reverse):

    def advance(carried, operands):
        block_state, block_total = operands
        return (jnp.exp(block_total)[..., None, None] * carried + block_state, carried)

    start_state = jnp.zeros(states.shape[1:], jnp.float32)
    return lax.scan(advance, start_state, (states, totals), reverse=reverse)


def mix_tokens(
    value_projected,
    key_projected,
    query_projected,
    output_gate_projected,
    step_projected_raw,
    head_decay_logarithm,
    position_extra_decay,
    value_filter_weight,
    key_filter_weight,
    query_filter_weight,
    head_norm_gain,
):
    tokens = value_projected.shape[0]
    value_width = value_projected.shape[1]
    key_width = key_projected.shape[1]
    head_count = step_projected_raw.shape[2]
    group_count = key_width // STATE
    per_group = head_count // group_count
    blocks = tokens // BLOCK
    joined = jnp.concatenate([value_projected, key_projected, query_projected], axis=1)
    padded = padded_2(joined, (TAPS - 1) // 2).astype(jnp.float32)
    weights = jnp.concatenate(
        [value_filter_weight, key_filter_weight, query_filter_weight], axis=1
    ).astype(jnp.float32)
    filtered = weights[0] * padded[0:tokens]
    for offset in range(1, TAPS):
        filtered = filtered + weights[offset] * padded[offset : offset + tokens]
    values = filtered[:, :value_width].astype(jnp.bfloat16)
    key_rows = jax.nn.silu(filtered[:, value_width : value_width + key_width]).astype(jnp.bfloat16)
    key_rows = key_rows.reshape(blocks, BLOCK, group_count, STATE)
    query_rows = jax.nn.silu(filtered[:, value_width + key_width :]).astype(jnp.bfloat16)
    query_rows = query_rows.reshape(blocks, BLOCK, group_count, STATE)
    positive_step_sizes = jax.nn.softplus(step_projected_raw.astype(jnp.float32))
    decay_logarithm = (
        -jnp.exp(head_decay_logarithm)[:, None, :] * positive_step_sizes
        + position_extra_decay[None]
    )
    scaled = (
        values.astype(jnp.float32).reshape(tokens, head_count, HEAD_DIM)[None]
        * positive_step_sizes[..., None]
    ).astype(jnp.bfloat16)
    scaled = scaled.reshape(2, blocks, BLOCK, group_count, per_group, HEAD_DIM)
    log_blocks = decay_logarithm.reshape(2, blocks, BLOCK, group_count, per_group)
    running = jnp.einsum("ls,dbsgh->dblgh", prefix_matrix(BLOCK), log_blocks, precision=highest)
    forward_cum = running[0]
    backward_excl = running[1] - log_blocks[1]
    forward_total = running[0][:, -1]
    backward_total = running[1][:, -1]
    scores = jnp.einsum("blgn,bsgn->blsg", query_rows, key_rows, preferred_element_type=jnp.float32)
    position = lax.broadcasted_iota(jnp.int32, (BLOCK,), 0)
    lower_mask = (position[None, :] <= position[:, None])[None, :, :, None, None]
    upper_mask = (position[None, :] >= position[:, None])[None, :, :, None, None]
    forward_gap = jnp.where(lower_mask, forward_cum[:, :, None] - forward_cum[:, None, :], -jnp.inf)
    backward_gap = jnp.where(
        upper_mask, backward_excl[:, None, :] - backward_excl[:, :, None], -jnp.inf
    )
    forward_weight = (scores[..., None] * jnp.exp(forward_gap)).astype(jnp.bfloat16)
    backward_weight = (scores[..., None] * jnp.exp(backward_gap)).astype(jnp.bfloat16)
    inner = jnp.einsum(
        "blsgh,bsghp->blghp", forward_weight, scaled[0], preferred_element_type=jnp.float32
    )
    inner = inner + jnp.einsum(
        "blsgh,bsghp->blghp", backward_weight, scaled[1], preferred_element_type=jnp.float32
    )
    key_wide = key_rows.astype(jnp.float32)[:, :, :, None, :]
    forward_keys = (jnp.exp(forward_total[:, None] - forward_cum)[..., None] * key_wide).astype(
        jnp.bfloat16
    )
    backward_keys = (jnp.exp(backward_excl)[..., None] * key_wide).astype(jnp.bfloat16)
    forward_state = jnp.einsum(
        "bsghn,bsghp->bghpn", forward_keys, scaled[0], preferred_element_type=jnp.float32
    )
    backward_state = jnp.einsum(
        "bsghn,bsghp->bghpn", backward_keys, scaled[1], preferred_element_type=jnp.float32
    )
    forward_final, forward_before = local_chain(forward_state, forward_total, False)
    backward_final, backward_before = local_chain(backward_state, backward_total, True)
    forward_sum = jnp.sum(forward_total, axis=0)
    backward_sum = jnp.sum(backward_total, axis=0)
    entering, leaving = carried_states(
        forward_sum, forward_final, backward_sum, backward_final
    )
    forward_prior = jnp.cumsum(forward_total, axis=0) - forward_total
    backward_after = backward_sum[None] - jnp.cumsum(backward_total, axis=0)
    forward_in = jnp.exp(forward_prior)[..., None, None] * entering[None] + forward_before
    backward_in = jnp.exp(backward_after)[..., None, None] * leaving[None] + backward_before
    forward_read = jnp.exp(forward_cum)[..., None] * jnp.einsum(
        "blgn,bghpn->blghp",
        query_rows,
        forward_in.astype(jnp.bfloat16),
        preferred_element_type=jnp.float32,
    )
    backward_read = jnp.exp(backward_total[:, None] - backward_excl)[..., None] * jnp.einsum(
        "blgn,bghpn->blghp",
        query_rows,
        backward_in.astype(jnp.bfloat16),
        preferred_element_type=jnp.float32,
    )
    mixer_raw = (inner + forward_read + backward_read).reshape(tokens, head_count, HEAD_DIM)
    gated = mixer_raw * jax.nn.silu(output_gate_projected.astype(jnp.float32)).reshape(
        tokens, head_count, HEAD_DIM
    )
    inverse_rms = lax.rsqrt(jnp.mean(gated * gated, axis=-1, keepdims=True) + epsilon)
    head_normed = (gated * inverse_rms * head_norm_gain.reshape(head_count, HEAD_DIM)).astype(
        jnp.bfloat16
    )
    return head_normed.reshape(tokens, head_count * HEAD_DIM)


def slot_table(route_rows, experts, capacity):
    flat_ids = route_rows.reshape(-1)
    expert_ids = lax.broadcasted_iota(jnp.int32, (flat_ids.shape[0], experts), 1)
    matches = (flat_ids[:, None] == expert_ids).astype(jnp.int32)
    earlier = jnp.cumsum(matches, axis=0) - matches
    rank_in = jnp.sum(matches * earlier, axis=1)
    return (flat_ids * capacity + rank_in).reshape(route_rows.shape)


def dispatch_rows(slots, token_rows, places):
    place_ids = lax.broadcasted_iota(jnp.int32, (places,) + slots.shape, 0)
    one_hot = jnp.sum((place_ids == slots[None]).astype(jnp.float32), axis=2).astype(jnp.bfloat16)
    return jnp.dot(one_hot, token_rows, preferred_element_type=jnp.float32).astype(jnp.bfloat16)


def shards(
    residual_layer_input,
    value_projected,
    key_projected,
    query_projected,
    output_gate_projected,
    step_projected_raw,
    head_decay_logarithm,
    position_extra_decay,
    value_filter_weight,
    key_filter_weight,
    query_filter_weight,
    head_norm_gain,
    mixer_output_matrix,
    expert_norm_gain,
    routes,
    chosen_expert_weight,
    expert_gate_matrix,
    expert_up_matrix,
    expert_down_matrix,
):
    heads_out = mix_tokens(
        value_projected,
        key_projected,
        query_projected,
        output_gate_projected,
        step_projected_raw,
        head_decay_logarithm,
        position_extra_decay,
        value_filter_weight,
        key_filter_weight,
        query_filter_weight,
        head_norm_gain,
    )
    projected = jnp.dot(
        gather_columns(heads_out, 4),
        mixer_output_matrix,
        preferred_element_type=jnp.float32,
    ).astype(jnp.bfloat16)
    tp = lax.axis_size("tp")
    (columns,) = exchange([projected.reshape(tp, -1, projected.shape[1])], "tp", 5)
    mixer_out = columns.swapaxes(0, 1).reshape(columns.shape[1], -1)
    middle = (residual_layer_input.astype(jnp.float32) + mixer_out.astype(jnp.float32)).astype(
        jnp.bfloat16
    )
    residual = middle.astype(jnp.float32)
    normed = (
        residual
        * lax.rsqrt(jnp.mean(residual * residual, axis=-1, keepdims=True) + epsilon)
        * expert_norm_gain
    ).astype(jnp.bfloat16)
    own_rows = normed.shape[0]
    model_width = normed.shape[1]
    top_count = routes.shape[1]
    experts = lax.axis_size("sp")
    capacity = 2 * own_rows * top_count // experts
    places = experts * capacity
    position = lax.axis_index("tp")
    own_routes = lax.dynamic_slice_in_dim(routes, position * own_rows, own_rows, 0)
    own_slots = slot_table(own_routes, experts, capacity)
    outgoing = dispatch_rows(own_slots, normed, places)
    slotted = outgoing.reshape(experts, capacity, model_width)
    if capacity % 16 == 0 and experts & (experts - 1) == 0 and experts >= 4:
        returned = run_experts(
            slotted, expert_gate_matrix, expert_up_matrix, expert_down_matrix, 6
        )
    else:
        arrived = spread_rows(slotted, 6)
        slot_rows = arrived.reshape(-1, model_width)
        gate_value = jnp.dot(slot_rows, expert_gate_matrix[0], preferred_element_type=jnp.float32)
        up_value = jnp.dot(slot_rows, expert_up_matrix[0], preferred_element_type=jnp.float32)
        hidden = (jax.nn.silu(gate_value) * up_value).astype(jnp.bfloat16)
        partial_sum = jnp.dot(hidden, expert_down_matrix[0], preferred_element_type=jnp.float32).astype(
            jnp.bfloat16
        )
        returned = collect_rows(partial_sum.reshape(arrived.shape), 7)
    chosen = (
        lax.broadcasted_iota(jnp.int32, (own_rows, top_count, places), 2) == own_slots[:, :, None]
    )
    mixing = jnp.sum(jnp.where(chosen, chosen_expert_weight[:, :, None], 0.0), axis=1)
    expert_mix = jnp.dot(
        mixing, returned.reshape(places, model_width).astype(jnp.float32), precision=highest
    )
    return (residual + expert_mix).astype(jnp.bfloat16)


def solution(mesh):
    return jax.shard_map(
        shards,
        mesh=mesh,
        in_specs=(
            P(("sp", "tp"), None),
            P("sp", "tp"),
            P("sp", "tp"),
            P("sp", "tp"),
            P("sp", "tp"),
            P(None, "sp", "tp"),
            P(None, "tp"),
            P("sp", "tp"),
            P(None, "tp"),
            P(None, "tp"),
            P(None, "tp"),
            P("tp"),
            P(None, "tp"),
            P(),
            P("sp", None),
            P(("sp", "tp"), None),
            P("sp", None, "tp"),
            P("sp", None, "tp"),
            P("sp", "tp", None),
        ),
        out_specs=P(("sp", "tp"), None),
        check_vma=False,
    )
```

```python
import functools

import jax
import jax.numpy as jnp
from jax import lax
from jax.experimental import pallas as pl
from jax.experimental.pallas import tpu as pltpu
from jax.sharding import PartitionSpec as P

HEAD_DIM = 64
STATE = 128
BLOCK = 128
TAPS = 5
LANES = 128


epsilon = 1e-06
highest = lax.Precision.HIGHEST


MESH = pl.DeviceIdType.MESH


def remote(src, dst, send, recv, device):
    return pltpu.make_async_remote_copy(
        src_ref=src,
        dst_ref=dst,
        send_sem=send,
        recv_sem=recv,
        device_id=device,
        device_id_type=MESH,
    )


def greet(devices):
    barrier = pltpu.get_barrier_semaphore()
    for device in devices:
        pl.semaphore_signal(barrier, inc=1, device_id=device, device_id_type=MESH)
    pl.semaphore_wait(barrier, len(devices))


def vmem(count):
    return [pl.BlockSpec(memory_space=pltpu.VMEM)] * count


def dma(*shape):
    return pltpu.SemaphoreType.DMA(shape)


def params(number):
    return pltpu.CompilerParams(collective_id=number, has_side_effects=True)


def each(count, body):
    lax.fori_loop(0, count, lambda k, _: (body(k), 0)[1], 0)


def exchange_kernel(axis, n, k, *refs):
    ins, outs = refs[:k], refs[k : 2 * k]
    send, recv, local = refs[2 * k :]
    me = lax.axis_index(axis)
    greet([{axis: lax.rem(me + d, n)} for d in range(1, n)])
    copies = []
    for d in range(1, n):
        peer = lax.rem(me + d, n)
        for a in range(k):
            copies.append(
                remote(ins[a].at[peer], outs[a].at[me], send.at[a, d], recv.at[a, d], {axis: peer})
            )
    for a in range(k):
        copies.append(pltpu.make_async_copy(ins[a].at[me], outs[a].at[me], local.at[a]))
    for copy in copies:
        copy.start()
    for copy in copies:
        copy.wait()


def exchange(arrays, axis, number):
    n, k = lax.axis_size(axis), len(arrays)
    return pl.pallas_call(
        functools.partial(exchange_kernel, axis, n, k),
        out_shape=[jax.ShapeDtypeStruct(a.shape, a.dtype) for a in arrays],
        in_specs=vmem(k),
        out_specs=vmem(k),
        scratch_shapes=[dma(k, n), dma(k, n), dma(k)],
        compiler_params=params(number),
    )(*arrays)


def edges_kernel(n, x, out, send, recv):
    me = lax.axis_index("sp")
    left, right = lax.rem(me + n - 1, n), lax.rem(me + 1, n)
    greet([{"sp": left}, {"sp": right}])
    copies = [
        remote(x.at[1], out.at[0], send.at[0], recv.at[0], {"sp": right}),
        remote(x.at[0], out.at[1], send.at[1], recv.at[1], {"sp": left}),
    ]
    for copy in copies:
        copy.start()
    for copy in copies:
        copy.wait()


def edges(x, number):
    return pl.pallas_call(
        functools.partial(edges_kernel, lax.axis_size("sp")),
        out_shape=jax.ShapeDtypeStruct(x.shape, x.dtype),
        in_specs=vmem(1),
        out_specs=vmem(1)[0],
        scratch_shapes=[dma(2), dma(2)],
        compiler_params=params(number),
    )(x)


def tp_places(tp):
    j = lax.axis_index("tp")
    core = lax.rem(j, 2)
    chip = lax.div(j, 2)
    return j, chip, core, tp // 2, chip * 2 + (1 - core)


def gather_kernel(tp, pieces, x, out, send, recv, rsend, rrecv, local):
    j, chip, core, chips, partner = tp_places(tp)
    width = x.shape[1]
    piece = x.shape[0] // pieces
    others = [lax.rem(chip + d, chips) * 2 + core for d in range(1, chips)]
    greet([{"tp": o} for o in others] + [{"tp": partner}])

    def place(b, r):
        return out.at[pl.ds(r * piece, piece), pl.ds(pl.multiple_of(b * width, 128), width)]

    own = pltpu.make_async_copy(
        x, out.at[:, pl.ds(pl.multiple_of(j * width, 128), width)], local.at[0]
    )
    own.start()
    waits = []
    for r in range(pieces):
        part = x.at[pl.ds(r * piece, piece)]
        for d in range(1, chips):
            copy = remote(part, place(j, r), send.at[r, d], recv.at[r, d], {"tp": others[d - 1]})
            copy.start()
            waits.append(copy)
    relays = []
    for r in range(pieces):
        part = x.at[pl.ds(r * piece, piece)]
        copy = remote(part, place(j, r), rsend.at[r, 0], rrecv.at[r, 0], {"tp": partner})
        copy.start()
        relays.append(copy)
    for r in range(pieces):
        for d in range(1, chips):
            came = lax.rem(chip + chips - d, chips) * 2 + core
            spot = place(came, r)
            remote(spot, spot, send.at[r, d], recv.at[r, d], {"tp": partner}).wait_recv()
            copy = remote(spot, spot, rsend.at[r, d], rrecv.at[r, d], {"tp": partner})
            copy.start()
            relays.append(copy)
    for copy in waits:
        copy.wait_send()
    for copy in relays:
        copy.wait()
    own.wait()


def gather_columns(x, number, pieces=2):
    tp = lax.axis_size("tp")
    sems = dma(pieces, tp // 2)
    return pl.pallas_call(
        functools.partial(gather_kernel, tp, pieces),
        out_shape=jax.ShapeDtypeStruct((x.shape[0], x.shape[1] * tp), x.dtype),
        in_specs=vmem(1),
        out_specs=vmem(1)[0],
        scratch_shapes=[sems, sems, sems, sems, dma(1)],
        compiler_params=params(number),
    )(x)


def spread_kernel(sp, tp, ahead, x, out, asend, arecv, fsend, frecv, rsend, rrecv, local):
    me = lax.axis_index("sp")
    j, chip, core, chips, partner = tp_places(tp)
    others = [lax.rem(chip + d, chips) * 2 + core for d in range(1, chips)]
    greet(
        [{"sp": lax.rem(me + d, sp)} for d in range(1, sp)]
        + [{"tp": o} for o in others]
        + [{"tp": partner}]
    )

    def across(d):
        peer = lax.rem(me + d, sp)
        return remote(x.at[peer], out.at[j, me], asend.at[d], arecv.at[d], {"sp": peer})

    def forward(d, k):
        spot = out.at[j, lax.rem(me + sp - d, sp)]
        return remote(spot, spot, fsend.at[d, k], frecv.at[d, k], {"tp": others[k - 1]})

    def relay(d, k):
        came = lax.rem(chip + chips - k, chips) * 2 + core
        spot = out.at[came, lax.rem(me + sp - d, sp)]
        return remote(spot, spot, rsend.at[d, k], rrecv.at[d, k], {"tp": partner})

    own = pltpu.make_async_copy(x.at[me], out.at[j, me], local.at[0])
    own.start()
    each(min(ahead, sp - 1), lambda d: across(d + 1).start())

    def onward(d):
        for k in range(1, chips):
            forward(d, k).start()
        relay(d, 0).start()

    def pass_on(d):
        for k in range(1, chips):
            forward(d, k).wait_recv()
            relay(d, k).start()

    own.wait()
    onward(0)

    def step(d):
        across(d + 1).wait_recv()

        @pl.when(d + 1 + ahead < sp)
        def _():
            across(d + 1 + ahead).start()

        onward(d + 1)
        pass_on(d)

    each(sp - 1, step)
    pass_on(sp - 1)

    def finish(d):
        for k in range(1, chips):
            forward(d, k).wait_send()
        for k in range(chips):
            relay(d, k).wait()

    each(sp, finish)
    each(sp - 1, lambda d: across(d + 1).wait_send())


def spread_rows(x, number):
    sp, tp = lax.axis_size("sp"), lax.axis_size("tp")
    pair = dma(sp, tp // 2)
    return pl.pallas_call(
        functools.partial(spread_kernel, sp, tp, 3),
        out_shape=jax.ShapeDtypeStruct((tp,) + x.shape, x.dtype),
        in_specs=vmem(1),
        out_specs=vmem(1)[0],
        scratch_shapes=[dma(sp), dma(sp), pair, pair, pair, pair, dma(1)],
        compiler_params=params(number),
    )(x)


def collect_kernel(
    sp, tp, x, out, first, joined, second, total, csend, crecv, fsend, frecv, asend, arecv, local
):
    me = lax.axis_index("sp")
    j, chip, core, chips, partner = tp_places(tp)
    others = [lax.rem(chip + d, chips) * 2 + core for d in range(1, chips)]
    greet(
        [{"sp": lax.rem(me + d, sp)} for d in range(1, sp)]
        + [{"tp": o} for o in others]
        + [{"tp": partner}]
    )

    def rows(d):
        return lax.rem(me + d, sp)

    def aim(k):
        return lax.rem(chip + k, chips)

    def beside(d, k):
        s = rows(d)
        return remote(
            x.at[aim(k) * 2 + (1 - core), s],
            first.at[k, s],
            csend.at[d, k],
            crecv.at[d, k],
            {"tp": partner},
        )

    def over(d, k):
        s = rows(d)
        return remote(
            joined.at[k, s], second.at[k, s], fsend.at[d, k], frecv.at[d, k], {"tp": others[k - 1]}
        )

    def back(d):
        s = rows(d)
        return remote(total.at[s], out.at[me], asend.at[d], arecv.at[d], {"sp": s})

    def begin(i):
        d = lax.rem(i + 1, sp)
        for k in range(chips):
            beside(d, lax.rem(k + 1, chips)).start()

    each(sp, begin)

    def join(d):
        s = rows(d)
        for k in range(1, chips):
            beside(d, k).wait_recv()
            mine = x[aim(k) * 2 + core, s].astype(jnp.float32)
            joined[k, s] = (mine + first[k, s].astype(jnp.float32)).astype(joined.dtype)
            over(d, k).start()

    def close(d):
        s = rows(d)
        beside(d, 0).wait_recv()
        value = x[j, s].astype(jnp.float32) + first[0, s].astype(jnp.float32)
        for k in range(1, chips):
            over(d, k).wait_recv()
            value = value + second[k, s].astype(jnp.float32)
        total[s] = value.astype(total.dtype)

    join(lax.rem(1, sp))

    def step(i):
        join(lax.rem(i + 2, sp))
        close(i + 1)
        back(i + 1).start()

    each(sp - 1, step)
    close(0)
    own = pltpu.make_async_copy(total.at[me], out.at[me], local.at[0])
    own.start()

    def finish(d):
        for k in range(chips):
            beside(d, k).wait_send()
        for k in range(1, chips):
            over(d, k).wait_send()

    each(sp, finish)
    each(sp - 1, lambda d: back(d + 1).wait())
    own.wait()


def collect_rows(x, number):
    sp, tp = lax.axis_size("sp"), lax.axis_size("tp")
    chips = tp // 2
    pair = dma(sp, chips)
    buffer = pltpu.VMEM((chips,) + x.shape[1:], x.dtype)
    return pl.pallas_call(
        functools.partial(collect_kernel, sp, tp),
        out_shape=jax.ShapeDtypeStruct(x.shape[1:], x.dtype),
        in_specs=vmem(1),
        out_specs=vmem(1)[0],
        scratch_shapes=[
            buffer,
            buffer,
            buffer,
            pltpu.VMEM(x.shape[1:], x.dtype),
            pair,
            pair,
            pair,
            pair,
            dma(sp),
            dma(sp),
            dma(1),
        ],
        compiler_params=params(number),
    )(x)


def flip(me, d):
    out, bit = me, 1
    while bit <= d:
        if d & bit:
            out = out + bit * (1 - 2 * lax.rem(lax.div(out, bit), 2))
        bit *= 2
    return out


def expert_kernel(
    sp, tp, x, wgate, wup, wdown, out,
    arr, part, hidden, first, joined, second, total, vgate, vup, vdown,
    asend, arecv, fsend, frecv, rsend, rrecv, csend, crecv, osend, orecv, bsend, brecv, local, load,
):
    me = lax.axis_index("sp")
    j, chip, core, chips, partner = tp_places(tp)
    others = [lax.rem(chip + d, chips) * 2 + core for d in range(1, chips)]
    cap, width = x.shape[1], x.shape[2]
    ff = vgate.shape[1]
    rows = 2 * tp * cap
    loads = [
        pltpu.make_async_copy(wgate.at[0], vgate, load.at[0]),
        pltpu.make_async_copy(wup.at[0], vup, load.at[1]),
        pltpu.make_async_copy(wdown.at[0], vdown, load.at[2]),
    ]
    for copy in loads:
        copy.start()
    own = pltpu.make_async_copy(x.at[me], arr.at[me, j], local.at[0])
    own.start()
    greet(
        [{"sp": flip(me, d)} for d in range(1, sp)]
        + [{"tp": o} for o in others]
        + [{"tp": partner}]
    )

    def across(d):
        peer = flip(me, d)
        return remote(x.at[peer], arr.at[me, j], asend.at[d], arecv.at[d], {"sp": peer})

    def forward(d, k):
        spot = arr.at[flip(me, d), j]
        return remote(spot, spot, fsend.at[d, k], frecv.at[d, k], {"tp": others[k - 1]})

    def relay(d, k):
        came = lax.rem(chip + chips - k, chips) * 2 + core
        spot = arr.at[flip(me, d), came]
        return remote(spot, spot, rsend.at[d, k], rrecv.at[d, k], {"tp": partner})

    def onward(d):
        if d == 0:
            own.wait()
        else:
            across(d).wait_recv()
        for k in range(1, chips):
            forward(d, k).start()
        relay(d, 0).start()

    def pass_on(d):
        for k in range(1, chips):
            forward(d, k).wait_recv()
            relay(d, k).start()

    def aim(k):
        return lax.rem(chip + k, chips)

    def beside(d, k):
        s = flip(me, d)
        return remote(
            part.at[s, aim(k) * 2 + (1 - core)],
            first.at[s, k],
            csend.at[d, k],
            crecv.at[d, k],
            {"tp": partner},
        )

    def over(d, k):
        s = flip(me, d)
        return remote(
            joined.at[s, k], second.at[s, k], osend.at[d, k], orecv.at[d, k], {"tp": others[k - 1]}
        )

    def back(d):
        s = flip(me, d)
        return remote(total.at[s], out.at[me], bsend.at[d], brecv.at[d], {"sp": s})

    def begin(d):
        for k in range(chips):
            beside(d, (k + 1) % chips).start()

    def join(d):
        s = flip(me, d)
        for k in range(1, chips):
            beside(d, k).wait_recv()
            mine = part[s, aim(k) * 2 + core].astype(jnp.float32)
            joined[s, k] = (mine + first[s, k].astype(jnp.float32)).astype(joined.dtype)
            over(d, k).start()

    def close(d):
        s = flip(me, d)
        beside(d, 0).wait_recv()
        value = part[s, j].astype(jnp.float32) + first[s, 0].astype(jnp.float32)
        for k in range(1, chips):
            over(d, k).wait_recv()
            value = value + second[s, k].astype(jnp.float32)
        if d == 0:
            out[me] = value.astype(out.dtype)
        else:
            total[s] = value.astype(total.dtype)
            back(d).start()

    tile = min(ff, 256)
    wide = min(width, 256)

    def gate_up(g):
        base = flip(me, 2 * g) - lax.rem(flip(me, 2 * g), 2)

        def step(f):
            cols = pl.ds(pl.multiple_of(f * tile, tile), tile)
            held = arr[pl.ds(base, 2)].reshape(rows, width)
            gate = jnp.dot(held, vgate[:, cols], preferred_element_type=jnp.float32)
            up = jnp.dot(held, vup[:, cols], preferred_element_type=jnp.float32)
            hidden[:, cols] = (gate / (1.0 + jnp.exp(-gate)) * up).astype(hidden.dtype)

        each(ff // tile, step)

    def down(g):
        base = flip(me, 2 * g) - lax.rem(flip(me, 2 * g), 2)

        def step(f):
            cols = pl.ds(pl.multiple_of(f * wide, wide), wide)
            value = jnp.dot(hidden[...], vdown[:, cols], preferred_element_type=jnp.float32)
            part[pl.ds(base, 2), :, :, cols] = value.astype(part.dtype).reshape(2, tp, cap, wide)

        each(width // wide, step)

    for d in range(1, sp):
        across(d).start()
    ahead = min(4, sp)
    onward(0)
    onward(1)
    onward(2)
    pass_on(0)
    onward(3)
    pass_on(1)
    for copy in loads[:2]:
        copy.wait()
    for g in range(sp // 2):
        for d in (2 * g, 2 * g + 1):
            if g > 0:
                pass_on(d)
        for d in (2 * g, 2 * g + 1):
            for k in range(chips):
                relay(d, k).wait_recv()
        gate_up(g)
        for d in (2 * g + ahead, 2 * g + ahead + 1):
            if d < sp:
                onward(d)
        if g == 0:
            loads[2].wait()
        down(g)
        begin(2 * g)
        begin(2 * g + 1)
        if g > 0:
            close(2 * g - 2)
            close(2 * g - 1)
        join(2 * g)
        join(2 * g + 1)
    close(sp - 2)
    close(sp - 1)
    for d in range(sp):
        for k in range(1, chips):
            forward(d, k).wait_send()
            over(d, k).wait_send()
        for k in range(chips):
            relay(d, k).wait_send()
            beside(d, k).wait_send()
        if d > 0:
            across(d).wait_send()
            back(d).wait()


def run_experts(x, wgate, wup, wdown, number):
    sp, tp = lax.axis_size("sp"), lax.axis_size("tp")
    chips = tp // 2
    cap, width = x.shape[1:]
    ff = wgate.shape[2]
    kind = x.dtype
    pair = dma(sp, chips)
    line = dma(sp)
    piece = pltpu.VMEM((sp, chips, cap, width), kind)
    return pl.pallas_call(
        functools.partial(expert_kernel, sp, tp),
        out_shape=jax.ShapeDtypeStruct(x.shape, kind),
        in_specs=vmem(1) + [pl.BlockSpec(memory_space=pl.ANY)] * 3,
        out_specs=vmem(1)[0],
        scratch_shapes=[
            pltpu.VMEM((sp, tp, cap, width), kind),
            pltpu.VMEM((sp, tp, cap, width), kind),
            pltpu.VMEM((2 * tp * cap, ff), kind),
            piece,
            piece,
            piece,
            pltpu.VMEM((sp, cap, width), kind),
            pltpu.VMEM(wgate.shape[1:], kind),
            pltpu.VMEM(wup.shape[1:], kind),
            pltpu.VMEM(wdown.shape[1:], kind),
            line, line, pair, pair, pair, pair, pair, pair, pair, pair, line, line, dma(1), dma(3),
        ],
        compiler_params=pltpu.CompilerParams(
            collective_id=number, has_side_effects=True, vmem_limit_bytes=56 * 2**20
        ),
    )(x, wgate, wup, wdown)


def padded_2(cells, width):
    count, here = lax.axis_size("sp"), lax.axis_index("sp")
    came = edges(jnp.stack([cells[:width], cells[-width:]]), 1)
    before = jnp.where(here > 0, came[0], jnp.zeros_like(came[0]))
    after = jnp.where(here < count - 1, came[1], jnp.zeros_like(came[1]))
    return jnp.concatenate([before, cells, after], axis=0)


def carried_states(forward_sum, forward_final, backward_sum, backward_final):
    count = lax.axis_size("sp")
    shape = forward_final.shape
    per_head = shape[-2]
    states = jnp.stack([forward_final, backward_final]).astype(jnp.bfloat16)
    states = states.reshape(2, count, -1, shape[-1]).swapaxes(0, 1)
    totals = jnp.stack([forward_sum, backward_sum]).reshape(2, -1)
    totals = jnp.repeat(totals, per_head, axis=1).reshape(2, count, -1).swapaxes(0, 1)
    states, totals = exchange([states, totals], "sp", 2)
    factors = jnp.exp(totals)[..., None]
    parts = states.astype(jnp.float32)
    forward, backward = [], []
    held = jnp.zeros(parts.shape[2:], jnp.float32)
    for s in range(count):
        forward.append(held)
        held = factors[s, 0] * held + parts[s, 0]
    held = jnp.zeros(parts.shape[2:], jnp.float32)
    for s in reversed(range(count)):
        backward.append(held)
        held = factors[s, 1] * held + parts[s, 1]
    both = jnp.stack([jnp.stack(forward), jnp.stack(backward[::-1])], axis=1)
    (both,) = exchange([both.astype(jnp.bfloat16)], "sp", 3)
    both = both.astype(jnp.float32)
    return both[:, 0].reshape(shape), both[:, 1].reshape(shape)


def prefix_matrix(length):
    row_index = lax.broadcasted_iota(jnp.int32, (length, length), 0)
    column_index = lax.broadcasted_iota(jnp.int32, (length, length), 1)
    return (column_index <= row_index).astype(jnp.float32)


def local_chain(states, totals, reverse):

    def advance(carried, operands):
        block_state, block_total = operands
        return (jnp.exp(block_total)[..., None, None] * carried + block_state, carried)

    start_state = jnp.zeros(states.shape[1:], jnp.float32)
    return lax.scan(advance, start_state, (states, totals), reverse=reverse)


def mix_tokens(
    value_projected,
    key_projected,
    query_projected,
    output_gate_projected,
    step_projected_raw,
    head_decay_logarithm,
    position_extra_decay,
    value_filter_weight,
    key_filter_weight,
    query_filter_weight,
    head_norm_gain,
):
    tokens = value_projected.shape[0]
    value_width = value_projected.shape[1]
    key_width = key_projected.shape[1]
    head_count = step_projected_raw.shape[2]
    group_count = key_width // STATE
    per_group = head_count // group_count
    blocks = tokens // BLOCK
    joined = jnp.concatenate([value_projected, key_projected, query_projected], axis=1)
    padded = padded_2(joined, (TAPS - 1) // 2).astype(jnp.float32)
    weights = jnp.concatenate(
        [value_filter_weight, key_filter_weight, query_filter_weight], axis=1
    ).astype(jnp.float32)
    filtered = weights[0] * padded[0:tokens]
    for offset in range(1, TAPS):
        filtered = filtered + weights[offset] * padded[offset : offset + tokens]
    values = filtered[:, :value_width].astype(jnp.bfloat16)
    key_rows = jax.nn.silu(filtered[:, value_width : value_width + key_width]).astype(jnp.bfloat16)
    key_rows = key_rows.reshape(blocks, BLOCK, group_count, STATE)
    query_rows = jax.nn.silu(filtered[:, value_width + key_width :]).astype(jnp.bfloat16)
    query_rows = query_rows.reshape(blocks, BLOCK, group_count, STATE)
    positive_step_sizes = jax.nn.softplus(step_projected_raw.astype(jnp.float32))
    decay_logarithm = (
        -jnp.exp(head_decay_logarithm)[:, None, :] * positive_step_sizes
        + position_extra_decay[None]
    )
    scaled = (
        values.astype(jnp.float32).reshape(tokens, head_count, HEAD_DIM)[None]
        * positive_step_sizes[..., None]
    ).astype(jnp.bfloat16)
    scaled = scaled.reshape(2, blocks, BLOCK, group_count, per_group, HEAD_DIM)
    log_blocks = decay_logarithm.reshape(2, blocks, BLOCK, group_count, per_group)
    running = jnp.einsum("ls,dbsgh->dblgh", prefix_matrix(BLOCK), log_blocks, precision=highest)
    forward_cum = running[0]
    backward_excl = running[1] - log_blocks[1]
    forward_total = running[0][:, -1]
    backward_total = running[1][:, -1]
    scores = jnp.einsum("blgn,bsgn->blsg", query_rows, key_rows, preferred_element_type=jnp.float32)
    position = lax.broadcasted_iota(jnp.int32, (BLOCK,), 0)
    lower_mask = (position[None, :] <= position[:, None])[None, :, :, None, None]
    upper_mask = (position[None, :] >= position[:, None])[None, :, :, None, None]
    forward_gap = jnp.where(lower_mask, forward_cum[:, :, None] - forward_cum[:, None, :], -jnp.inf)
    backward_gap = jnp.where(
        upper_mask, backward_excl[:, None, :] - backward_excl[:, :, None], -jnp.inf
    )
    forward_weight = (scores[..., None] * jnp.exp(forward_gap)).astype(jnp.bfloat16)
    backward_weight = (scores[..., None] * jnp.exp(backward_gap)).astype(jnp.bfloat16)
    inner = jnp.einsum(
        "blsgh,bsghp->blghp", forward_weight, scaled[0], preferred_element_type=jnp.float32
    )
    inner = inner + jnp.einsum(
        "blsgh,bsghp->blghp", backward_weight, scaled[1], preferred_element_type=jnp.float32
    )
    key_wide = key_rows.astype(jnp.float32)[:, :, :, None, :]
    forward_keys = (jnp.exp(forward_total[:, None] - forward_cum)[..., None] * key_wide).astype(
        jnp.bfloat16
    )
    backward_keys = (jnp.exp(backward_excl)[..., None] * key_wide).astype(jnp.bfloat16)
    forward_state = jnp.einsum(
        "bsghn,bsghp->bghpn", forward_keys, scaled[0], preferred_element_type=jnp.float32
    )
    backward_state = jnp.einsum(
        "bsghn,bsghp->bghpn", backward_keys, scaled[1], preferred_element_type=jnp.float32
    )
    forward_final, forward_before = local_chain(forward_state, forward_total, False)
    backward_final, backward_before = local_chain(backward_state, backward_total, True)
    forward_sum = jnp.sum(forward_total, axis=0)
    backward_sum = jnp.sum(backward_total, axis=0)
    entering, leaving = carried_states(
        forward_sum, forward_final, backward_sum, backward_final
    )
    forward_prior = jnp.cumsum(forward_total, axis=0) - forward_total
    backward_after = backward_sum[None] - jnp.cumsum(backward_total, axis=0)
    forward_in = jnp.exp(forward_prior)[..., None, None] * entering[None] + forward_before
    backward_in = jnp.exp(backward_after)[..., None, None] * leaving[None] + backward_before
    forward_read = jnp.exp(forward_cum)[..., None] * jnp.einsum(
        "blgn,bghpn->blghp",
        query_rows,
        forward_in.astype(jnp.bfloat16),
        preferred_element_type=jnp.float32,
    )
    backward_read = jnp.exp(backward_total[:, None] - backward_excl)[..., None] * jnp.einsum(
        "blgn,bghpn->blghp",
        query_rows,
        backward_in.astype(jnp.bfloat16),
        preferred_element_type=jnp.float32,
    )
    mixer_raw = (inner + forward_read + backward_read).reshape(tokens, head_count, HEAD_DIM)
    gated = mixer_raw * jax.nn.silu(output_gate_projected.astype(jnp.float32)).reshape(
        tokens, head_count, HEAD_DIM
    )
    inverse_rms = lax.rsqrt(jnp.mean(gated * gated, axis=-1, keepdims=True) + epsilon)
    head_normed = (gated * inverse_rms * head_norm_gain.reshape(head_count, HEAD_DIM)).astype(
        jnp.bfloat16
    )
    return head_normed.reshape(tokens, head_count * HEAD_DIM)


def mixer_kernel(
    n, span, value, key, query, gate, raw, rate, extra, vfilter, kfilter, qfilter, gain, out,
    hv, hk, hq, pad, vals, keys, queries, turned, column, lines, totals, inner, weight,
    fin, met, came, gone, held, given, result,
    esend, erecv, tsend, trecv, xsend, xrecv, zsend, zrecv, ysend, yrecv,
):
    me = lax.axis_index("sp")
    b, a = lax.rem(me, 2), lax.div(me, 2)
    beside, planes = me + 1 - 2 * b, n // 2
    tokens, wide = value.shape
    heads = raw.shape[2]
    groups = key.shape[1] // STATE
    tiles = wide // LANES
    per = tiles // groups
    half = tiles // 2
    chunks = half // span
    f32 = jnp.float32

    edge = hv.shape[1]
    arrays = [(value, hv), (key, hk), (query, hq)]

    def edge_copy(i, way):
        src, halo = arrays[i]
        start, peer = (tokens - edge, lax.rem(me + 1, n)) if way == 0 else (0, lax.rem(me + n - 1, n))
        return remote(
            src.at[pl.ds(start, edge)], halo.at[way], esend.at[i, way], erecv.at[i, way], {"sp": peer}
        )

    greet([{"sp": lax.rem(me + d, n)} for d in range(1, n)])
    sends = [me < n - 1, me > 0]
    waits = [me > 0, me < n - 1]
    for way in range(2):

        @pl.when(sends[way])
        def _():
            for i in range(3):
                edge_copy(i, way).start()

        @pl.when(jnp.logical_not(waits[way]))
        def _():
            for _, halo in arrays:
                halo[way] = jnp.zeros(halo.shape[1:], halo.dtype)

    row = lax.broadcasted_iota(jnp.int32, (tokens, tokens), 0)
    col = lax.broadcasted_iota(jnp.int32, (tokens, tokens), 1)
    prefix = (col <= row).astype(f32)
    column[...] = jnp.zeros(column.shape, f32)
    lane = lax.broadcasted_iota(jnp.int32, (tokens, LANES), 1)
    for d in range(2):
        r = raw[d].astype(f32)
        step = jnp.maximum(r, 0.0) + jnp.log1p(jnp.exp(-jnp.abs(r)))
        decay = -jnp.exp(rate[pl.ds(d, 1), :]) * step + extra[...]
        total = jnp.dot(prefix, decay, preferred_element_type=f32, precision=highest)
        last = total[tokens - 1 : tokens, :]
        part = total if d == 0 else total - decay
        gap = last - total if d == 0 else part
        read = total if d == 0 else last - part
        column[d, :, 0:heads] = part
        column[2 + d, :, 0:heads] = step
        column[4 + d, :, 0:heads] = jnp.exp(gap) * step
        column[6 + d, :, 0:heads] = jnp.exp(read)
        totals[0, d, :, :] = jnp.zeros(totals.shape[2:], f32)
        totals[0, d, :, 0:heads] = jnp.broadcast_to(jnp.exp(last), (8, heads))
    for q in range(4):
        lines[q] = column[q].T

    def total_copy():
        return remote(totals.at[0], totals.at[1], tsend.at[0], trecv.at[0], {"sp": beside})

    total_copy().start()

    for way in range(2):

        @pl.when(waits[way])
        def _():
            for i in range(3):
                edge_copy(i, way).wait_recv()

    def convolve(src, halo, taps, store):
        reach = (TAPS - 1) // 2

        def step(i):
            cols = pl.ds(pl.multiple_of(i * LANES, LANES), LANES)
            pad[pl.ds(8, tokens)] = src[:, cols].astype(f32)
            pad[pl.ds(0, 8)] = halo[0, :, cols].astype(f32)[edge - 8 :]
            pad[pl.ds(8 + tokens, 8)] = halo[1, :, cols].astype(f32)[:8]
            w = taps[:, cols].astype(f32)
            acc = w[0:1] * pad[pl.ds(8 - reach, tokens)]
            for o in range(1, TAPS):
                acc = acc + w[o : o + 1] * pad[pl.ds(8 - reach + o, tokens)]
            store(i, cols, acc)

        each(src.shape[1] // LANES, step)

    def silu(v):
        return v / (1.0 + jnp.exp(-v))

    def keep_values(i, cols, acc):
        vals[:, cols] = acc.astype(vals.dtype)

    def keep_keys(i, cols, acc):
        acc = silu(acc)
        keys[:, cols] = acc.astype(keys.dtype)
        turned[i] = acc.T.astype(turned.dtype)

    def keep_queries(i, cols, acc):
        queries[:, cols] = silu(acc).astype(queries.dtype)

    convolve(value, hv, vfilter, keep_values)
    convolve(key, hk, kfilter, keep_keys)

    def spread(x, k):
        low, high = x[:, k : k + 1], x[:, k + 1 : k + 2]
        return jnp.where(lane[: x.shape[0]] < HEAD_DIM, low, high)

    def shifted(q, first):
        return pltpu.roll(column[q], lax.rem(LANES - first, LANES), 1)

    def cross(d, c):
        spot = pl.ds((1 - b) * half + c * span, span)
        mine = pl.ds(b * half + c * span, span)
        return (
            remote(fin.at[d, spot], met.at[d, pl.ds(c * span, span)], xsend.at[d, c], xrecv.at[d, c], {"sp": beside}),
            mine,
        )

    def states(i):
        g = lax.rem(i + (1 - b) * (groups // 2), groups)
        for d in range(2):
            scale = shifted(4 + d, g * 2 * per)
            for k in range(per):
                cols = pl.ds(pl.multiple_of((g * per + k) * LANES, LANES), LANES)
                scaled = (vals[:, cols].astype(f32) * spread(scale, 2 * k)).astype(vals.dtype)
                fin[d, g * per + k] = jnp.dot(
                    turned[g], scaled, preferred_element_type=f32
                ).astype(fin.dtype)

    each(groups, states)
    for c in range(chunks):
        for d in range(2):
            cross(d, c)[0].start()
    convolve(query, hq, qfilter, keep_queries)

    block_row = lax.broadcasted_iota(jnp.int32, (BLOCK, BLOCK), 0)
    block_col = lax.broadcasted_iota(jnp.int32, (BLOCK, BLOCK), 1)

    def within(g):
        kcols = pl.ds(pl.multiple_of(g * STATE, STATE), STATE)
        scores = lax.dot_general(
            queries[:, kcols], keys[:, kcols], (((1,), (1,)), ((), ())), preferred_element_type=f32
        )
        first = g * 2 * per
        ahead, behind = shifted(0, first), shifted(1, first)
        for k in range(2 * per):
            fr, er = lines[0, pl.ds(first + k, 1), :], lines[1, pl.ds(first + k, 1), :]
            sf, sb = lines[2, pl.ds(first + k, 1), :], lines[3, pl.ds(first + k, 1), :]
            for i in range(tokens // BLOCK):
                rows = slice(i * BLOCK, (i + 1) * BLOCK)
                fc = jnp.broadcast_to(ahead[rows, k : k + 1], (BLOCK, BLOCK))
                ec = jnp.broadcast_to(behind[rows, k : k + 1], (BLOCK, BLOCK))
                for m in range(tokens // BLOCK):
                    cols = slice(m * BLOCK, (m + 1) * BLOCK)
                    if m < i:
                        gap, size = fc - fr[:, cols], sf[:, cols]
                    elif m > i:
                        gap, size = er[:, cols] - ec, sb[:, cols]
                    else:
                        lower, upper = block_col <= block_row, block_col >= block_row
                        gap = jnp.where(lower, fc - fr[:, cols], er[:, cols] - ec)
                        size = jnp.where(lower, sf[:, cols], 0.0) + jnp.where(upper, sb[:, cols], 0.0)
                    weight[k % 2, rows, cols] = (scores[rows, cols] * jnp.exp(gap) * size).astype(
                        weight.dtype
                    )
            if k % 2 == 1:
                spot = pl.ds(pl.multiple_of((g * per + k // 2) * LANES, LANES), LANES)
                both = vals[:, spot]
                low = jnp.dot(weight[0], both, preferred_element_type=f32)
                high = jnp.dot(weight[1], both, preferred_element_type=f32)
                inner[:, spot] = jnp.where(lane < HEAD_DIM, low, high)

    each(groups, within)

    total_copy().wait()
    factor = [pltpu.roll(totals[i, d], lax.rem(LANES - 2 * b * half, LANES), 1) for i in range(2) for d in range(2)]
    early = b == 0

    def chain(d, c):
        peer = lax.rem(me + (2 if d == 0 else n - 2), n)
        spot = pl.ds(c * span, span)
        return remote(gone.at[d, spot], came.at[d, spot], zsend.at[d, c], zrecv.at[d, c], {"sp": peer})

    def answer(d, c):
        there = pl.ds(b * half + c * span, span)
        return remote(
            given.at[d, pl.ds(c * span, span)], result.at[d, there], ysend.at[d, c], yrecv.at[d, c], {"sp": beside}
        )

    def answered(d, c):
        there = pl.ds((1 - b) * half + c * span, span)
        return remote(
            given.at[d, pl.ds(c * span, span)], result.at[d, there], ysend.at[d, c], yrecv.at[d, c], {"sp": beside}
        )

    for c in range(chunks):
        for d in range(2):
            cross(d, c)[0].wait_recv()
            starts = a == 0 if d == 0 else a == planes - 1
            ends = a == planes - 1 if d == 0 else a == 0

            @pl.when(starts)
            def _():
                came[d, pl.ds(c * span, span)] = jnp.zeros((span,) + came.shape[2:], came.dtype)

            @pl.when(jnp.logical_not(starts))
            def _():
                chain(d, c).wait_recv()

            for k in range(span):
                u = c * span + k
                mine = spread(factor[d], 2 * u)[0:1]
                other = spread(factor[2 + d], 2 * u)[0:1]
                state = came[d, u].astype(f32)
                own = fin[d, b * half + u].astype(f32)
                got = met[d, u].astype(f32)
                near_first = early if d == 0 else jnp.logical_not(early)
                head = jnp.where(near_first, own, got)
                tail = jnp.where(near_first, got, own)
                head_factor = jnp.where(near_first, mine, other)
                tail_factor = jnp.where(near_first, other, mine)
                middle = head_factor * state + head
                gone[d, u] = (tail_factor * middle + tail).astype(gone.dtype)
                held[d, u] = jnp.where(near_first, state, middle).astype(held.dtype)
                given[d, u] = jnp.where(near_first, middle, state).astype(given.dtype)

            @pl.when(jnp.logical_not(ends))
            def _():
                chain(d, c).start()

            answer(d, c).start()
            result[d, pl.ds(b * half + c * span, span)] = held[d, pl.ds(c * span, span)]

    block = lax.broadcasted_iota(jnp.int32, (LANES, LANES), 0) // HEAD_DIM
    share = jnp.where(
        block == lax.broadcasted_iota(jnp.int32, (LANES, LANES), 1) // HEAD_DIM, 1.0 / HEAD_DIM, 0.0
    ).astype(vals.dtype)

    def finish(u):
        g = lax.div(u, per)
        kcols = pl.ds(pl.multiple_of(g * STATE, STATE), STATE)
        cols = pl.ds(pl.multiple_of(u * LANES, LANES), LANES)
        q = queries[:, kcols]
        mixed = inner[:, cols]
        for d in range(2):
            carried = jnp.dot(q, result[d, u], preferred_element_type=f32)
            mixed = mixed + spread(shifted(6 + d, 2 * u), 0) * carried
        gated = mixed * silu(gate[:, cols].astype(f32))
        square = gated * gated
        top = square.astype(share.dtype)
        rest = (square - top.astype(f32)).astype(share.dtype)
        mean = jnp.dot(top, share, preferred_element_type=f32)
        mean = mean + jnp.dot(rest, share, preferred_element_type=f32)
        out[:, cols] = (gated * lax.rsqrt(mean + epsilon) * gain[:, cols]).astype(out.dtype)

    each(half, lambda u: finish(b * half + u))
    for c in range(chunks):
        for d in range(2):
            answered(d, c).wait_recv()
    each(half, lambda u: finish((1 - b) * half + u))

    for way in range(2):

        @pl.when(sends[way])
        def _():
            for i in range(3):
                edge_copy(i, way).wait_send()

    for c in range(chunks):
        for d in range(2):
            ends = a == planes - 1 if d == 0 else a == 0
            cross(d, c)[0].wait_send()
            answer(d, c).wait_send()

            @pl.when(jnp.logical_not(ends))
            def _():
                chain(d, c).wait_send()


def run_mixer(
    value, key, query, gate, raw, rate, extra, vfilter, kfilter, qfilter, gain, number
):
    n = lax.axis_size("sp")
    tokens, wide = value.shape
    narrow = key.shape[1]
    groups, tiles = narrow // STATE, wide // LANES
    half = tiles // 2
    span = 2 if half % 2 == 0 else 1
    kind, f32 = value.dtype, jnp.float32
    edge = 16
    state = pltpu.VMEM((2, half, STATE, LANES), kind)
    full = pltpu.VMEM((2, tiles, STATE, LANES), kind)
    sems = dma(2, half // span)
    return pl.pallas_call(
        functools.partial(mixer_kernel, n, span),
        out_shape=jax.ShapeDtypeStruct((tokens, wide), kind),
        in_specs=vmem(11),
        out_specs=vmem(1)[0],
        scratch_shapes=[
            pltpu.VMEM((2, edge, wide), kind),
            pltpu.VMEM((2, edge, narrow), kind),
            pltpu.VMEM((2, edge, narrow), kind),
            pltpu.VMEM((tokens + 16, LANES), f32),
            pltpu.VMEM((tokens, wide), kind),
            pltpu.VMEM((tokens, narrow), kind),
            pltpu.VMEM((tokens, narrow), kind),
            pltpu.VMEM((groups, STATE, tokens), kind),
            pltpu.VMEM((8, tokens, LANES), f32),
            pltpu.VMEM((4, LANES, tokens), f32),
            pltpu.VMEM((2, 2, 8, LANES), f32),
            pltpu.VMEM((tokens, wide), f32),
            pltpu.VMEM((2, tokens, tokens), kind),
            full, state, state, state, state, state, full,
            dma(3, 2), dma(3, 2), dma(1), dma(1), sems, sems, sems, sems, sems, sems,
        ],
        compiler_params=pltpu.CompilerParams(
            collective_id=number, has_side_effects=True, vmem_limit_bytes=40 * 2**20
        ),
    )(value, key, query, gate, raw, rate, extra, vfilter, kfilter, qfilter, gain.reshape(1, -1))


def slot_table(route_rows, experts, capacity):
    flat_ids = route_rows.reshape(-1)
    expert_ids = lax.broadcasted_iota(jnp.int32, (flat_ids.shape[0], experts), 1)
    matches = (flat_ids[:, None] == expert_ids).astype(jnp.int32)
    earlier = jnp.cumsum(matches, axis=0) - matches
    rank_in = jnp.sum(matches * earlier, axis=1)
    return (flat_ids * capacity + rank_in).reshape(route_rows.shape)


def dispatch_rows(slots, token_rows, places):
    place_ids = lax.broadcasted_iota(jnp.int32, (places,) + slots.shape, 0)
    one_hot = jnp.sum((place_ids == slots[None]).astype(jnp.float32), axis=2).astype(jnp.bfloat16)
    return jnp.dot(one_hot, token_rows, preferred_element_type=jnp.float32).astype(jnp.bfloat16)


def shards(
    residual_layer_input,
    value_projected,
    key_projected,
    query_projected,
    output_gate_projected,
    step_projected_raw,
    head_decay_logarithm,
    position_extra_decay,
    value_filter_weight,
    key_filter_weight,
    query_filter_weight,
    head_norm_gain,
    mixer_output_matrix,
    expert_norm_gain,
    routes,
    chosen_expert_weight,
    expert_gate_matrix,
    expert_up_matrix,
    expert_down_matrix,
):
    operands = (
        value_projected,
        key_projected,
        query_projected,
        output_gate_projected,
        step_projected_raw,
        head_decay_logarithm,
        position_extra_decay,
        value_filter_weight,
        key_filter_weight,
        query_filter_weight,
        head_norm_gain,
    )
    if value_projected.shape[1] % (2 * LANES) == 0 and lax.axis_size("sp") % 2 == 0:
        heads_out = run_mixer(*operands, 2)
    else:
        heads_out = mix_tokens(*operands)
    projected = jnp.dot(
        gather_columns(heads_out, 4),
        mixer_output_matrix,
        preferred_element_type=jnp.float32,
    ).astype(jnp.bfloat16)
    tp = lax.axis_size("tp")
    (columns,) = exchange([projected.reshape(tp, -1, projected.shape[1])], "tp", 5)
    mixer_out = columns.swapaxes(0, 1).reshape(columns.shape[1], -1)
    middle = (residual_layer_input.astype(jnp.float32) + mixer_out.astype(jnp.float32)).astype(
        jnp.bfloat16
    )
    residual = middle.astype(jnp.float32)
    normed = (
        residual
        * lax.rsqrt(jnp.mean(residual * residual, axis=-1, keepdims=True) + epsilon)
        * expert_norm_gain
    ).astype(jnp.bfloat16)
    own_rows = normed.shape[0]
    model_width = normed.shape[1]
    top_count = routes.shape[1]
    experts = lax.axis_size("sp")
    capacity = 2 * own_rows * top_count // experts
    places = experts * capacity
    position = lax.axis_index("tp")
    own_routes = lax.dynamic_slice_in_dim(routes, position * own_rows, own_rows, 0)
    own_slots = slot_table(own_routes, experts, capacity)
    outgoing = dispatch_rows(own_slots, normed, places)
    slotted = outgoing.reshape(experts, capacity, model_width)
    if capacity % 16 == 0 and experts & (experts - 1) == 0 and experts >= 4:
        returned = run_experts(
            slotted, expert_gate_matrix, expert_up_matrix, expert_down_matrix, 6
        )
    else:
        arrived = spread_rows(slotted, 6)
        slot_rows = arrived.reshape(-1, model_width)
        gate_value = jnp.dot(slot_rows, expert_gate_matrix[0], preferred_element_type=jnp.float32)
        up_value = jnp.dot(slot_rows, expert_up_matrix[0], preferred_element_type=jnp.float32)
        hidden = (jax.nn.silu(gate_value) * up_value).astype(jnp.bfloat16)
        partial_sum = jnp.dot(hidden, expert_down_matrix[0], preferred_element_type=jnp.float32).astype(
            jnp.bfloat16
        )
        returned = collect_rows(partial_sum.reshape(arrived.shape), 7)
    chosen = (
        lax.broadcasted_iota(jnp.int32, (own_rows, top_count, places), 2) == own_slots[:, :, None]
    )
    mixing = jnp.sum(jnp.where(chosen, chosen_expert_weight[:, :, None], 0.0), axis=1)
    expert_mix = jnp.dot(
        mixing, returned.reshape(places, model_width).astype(jnp.float32), precision=highest
    )
    return (residual + expert_mix).astype(jnp.bfloat16)


def solution(mesh):
    return jax.shard_map(
        shards,
        mesh=mesh,
        in_specs=(
            P(("sp", "tp"), None),
            P("sp", "tp"),
            P("sp", "tp"),
            P("sp", "tp"),
            P("sp", "tp"),
            P(None, "sp", "tp"),
            P(None, "tp"),
            P("sp", "tp"),
            P(None, "tp"),
            P(None, "tp"),
            P(None, "tp"),
            P("tp"),
            P(None, "tp"),
            P(),
            P("sp", None),
            P(("sp", "tp"), None),
            P("sp", None, "tp"),
            P("sp", None, "tp"),
            P("sp", "tp", None),
        ),
        out_specs=P(("sp", "tp"), None),
        check_vma=False,
    )
```

```python
import functools

import jax
import jax.numpy as jnp
from jax import lax
from jax.experimental import pallas as pl
from jax.experimental.pallas import tpu as pltpu
from jax.sharding import PartitionSpec as P

HEAD_DIM = 64
STATE = 128
BLOCK = 128
TAPS = 5
LANES = 128


epsilon = 1e-06
highest = lax.Precision.HIGHEST


MESH = pl.DeviceIdType.MESH


def remote(src, dst, send, recv, device):
    return pltpu.make_async_remote_copy(
        src_ref=src,
        dst_ref=dst,
        send_sem=send,
        recv_sem=recv,
        device_id=device,
        device_id_type=MESH,
    )


def greet(devices):
    barrier = pltpu.get_barrier_semaphore()
    for device in devices:
        pl.semaphore_signal(barrier, inc=1, device_id=device, device_id_type=MESH)
    pl.semaphore_wait(barrier, len(devices))


def vmem(count):
    return [pl.BlockSpec(memory_space=pltpu.VMEM)] * count


def dma(*shape):
    return pltpu.SemaphoreType.DMA(shape)


def params(number):
    return pltpu.CompilerParams(collective_id=number, has_side_effects=True)


def each(count, body):
    lax.fori_loop(0, count, lambda k, _: (body(k), 0)[1], 0)


def exchange_kernel(axis, n, k, *refs):
    ins, outs = refs[:k], refs[k : 2 * k]
    send, recv, local = refs[2 * k :]
    me = lax.axis_index(axis)
    greet([{axis: lax.rem(me + d, n)} for d in range(1, n)])
    copies = []
    for d in range(1, n):
        peer = lax.rem(me + d, n)
        for a in range(k):
            copies.append(
                remote(ins[a].at[peer], outs[a].at[me], send.at[a, d], recv.at[a, d], {axis: peer})
            )
    for a in range(k):
        copies.append(pltpu.make_async_copy(ins[a].at[me], outs[a].at[me], local.at[a]))
    for copy in copies:
        copy.start()
    for copy in copies:
        copy.wait()


def exchange(arrays, axis, number):
    n, k = lax.axis_size(axis), len(arrays)
    return pl.pallas_call(
        functools.partial(exchange_kernel, axis, n, k),
        out_shape=[jax.ShapeDtypeStruct(a.shape, a.dtype) for a in arrays],
        in_specs=vmem(k),
        out_specs=vmem(k),
        scratch_shapes=[dma(k, n), dma(k, n), dma(k)],
        compiler_params=params(number),
    )(*arrays)


def edges_kernel(n, x, out, send, recv):
    me = lax.axis_index("sp")
    left, right = lax.rem(me + n - 1, n), lax.rem(me + 1, n)
    greet([{"sp": left}, {"sp": right}])
    copies = [
        remote(x.at[1], out.at[0], send.at[0], recv.at[0], {"sp": right}),
        remote(x.at[0], out.at[1], send.at[1], recv.at[1], {"sp": left}),
    ]
    for copy in copies:
        copy.start()
    for copy in copies:
        copy.wait()


def edges(x, number):
    return pl.pallas_call(
        functools.partial(edges_kernel, lax.axis_size("sp")),
        out_shape=jax.ShapeDtypeStruct(x.shape, x.dtype),
        in_specs=vmem(1),
        out_specs=vmem(1)[0],
        scratch_shapes=[dma(2), dma(2)],
        compiler_params=params(number),
    )(x)


def tp_places(tp):
    j = lax.axis_index("tp")
    core = lax.rem(j, 2)
    chip = lax.div(j, 2)
    return j, chip, core, tp // 2, chip * 2 + (1 - core)


def gather_kernel(tp, pieces, x, out, send, recv, rsend, rrecv, local):
    j, chip, core, chips, partner = tp_places(tp)
    width = x.shape[1]
    piece = x.shape[0] // pieces
    others = [lax.rem(chip + d, chips) * 2 + core for d in range(1, chips)]
    greet([{"tp": o} for o in others] + [{"tp": partner}])

    def place(b, r):
        return out.at[pl.ds(r * piece, piece), pl.ds(pl.multiple_of(b * width, 128), width)]

    own = pltpu.make_async_copy(
        x, out.at[:, pl.ds(pl.multiple_of(j * width, 128), width)], local.at[0]
    )
    own.start()
    waits = []
    for r in range(pieces):
        part = x.at[pl.ds(r * piece, piece)]
        for d in range(1, chips):
            copy = remote(part, place(j, r), send.at[r, d], recv.at[r, d], {"tp": others[d - 1]})
            copy.start()
            waits.append(copy)
    relays = []
    for r in range(pieces):
        part = x.at[pl.ds(r * piece, piece)]
        copy = remote(part, place(j, r), rsend.at[r, 0], rrecv.at[r, 0], {"tp": partner})
        copy.start()
        relays.append(copy)
    for r in range(pieces):
        for d in range(1, chips):
            came = lax.rem(chip + chips - d, chips) * 2 + core
            spot = place(came, r)
            remote(spot, spot, send.at[r, d], recv.at[r, d], {"tp": partner}).wait_recv()
            copy = remote(spot, spot, rsend.at[r, d], rrecv.at[r, d], {"tp": partner})
            copy.start()
            relays.append(copy)
    for copy in waits:
        copy.wait_send()
    for copy in relays:
        copy.wait()
    own.wait()


def gather_columns(x, number, pieces=2):
    tp = lax.axis_size("tp")
    sems = dma(pieces, tp // 2)
    return pl.pallas_call(
        functools.partial(gather_kernel, tp, pieces),
        out_shape=jax.ShapeDtypeStruct((x.shape[0], x.shape[1] * tp), x.dtype),
        in_specs=vmem(1),
        out_specs=vmem(1)[0],
        scratch_shapes=[sems, sems, sems, sems, dma(1)],
        compiler_params=params(number),
    )(x)


def spread_kernel(sp, tp, ahead, x, out, asend, arecv, fsend, frecv, rsend, rrecv, local):
    me = lax.axis_index("sp")
    j, chip, core, chips, partner = tp_places(tp)
    others = [lax.rem(chip + d, chips) * 2 + core for d in range(1, chips)]
    greet(
        [{"sp": lax.rem(me + d, sp)} for d in range(1, sp)]
        + [{"tp": o} for o in others]
        + [{"tp": partner}]
    )

    def across(d):
        peer = lax.rem(me + d, sp)
        return remote(x.at[peer], out.at[j, me], asend.at[d], arecv.at[d], {"sp": peer})

    def forward(d, k):
        spot = out.at[j, lax.rem(me + sp - d, sp)]
        return remote(spot, spot, fsend.at[d, k], frecv.at[d, k], {"tp": others[k - 1]})

    def relay(d, k):
        came = lax.rem(chip + chips - k, chips) * 2 + core
        spot = out.at[came, lax.rem(me + sp - d, sp)]
        return remote(spot, spot, rsend.at[d, k], rrecv.at[d, k], {"tp": partner})

    own = pltpu.make_async_copy(x.at[me], out.at[j, me], local.at[0])
    own.start()
    each(min(ahead, sp - 1), lambda d: across(d + 1).start())

    def onward(d):
        for k in range(1, chips):
            forward(d, k).start()
        relay(d, 0).start()

    def pass_on(d):
        for k in range(1, chips):
            forward(d, k).wait_recv()
            relay(d, k).start()

    own.wait()
    onward(0)

    def step(d):
        across(d + 1).wait_recv()

        @pl.when(d + 1 + ahead < sp)
        def _():
            across(d + 1 + ahead).start()

        onward(d + 1)
        pass_on(d)

    each(sp - 1, step)
    pass_on(sp - 1)

    def finish(d):
        for k in range(1, chips):
            forward(d, k).wait_send()
        for k in range(chips):
            relay(d, k).wait()

    each(sp, finish)
    each(sp - 1, lambda d: across(d + 1).wait_send())


def spread_rows(x, number):
    sp, tp = lax.axis_size("sp"), lax.axis_size("tp")
    pair = dma(sp, tp // 2)
    return pl.pallas_call(
        functools.partial(spread_kernel, sp, tp, 3),
        out_shape=jax.ShapeDtypeStruct((tp,) + x.shape, x.dtype),
        in_specs=vmem(1),
        out_specs=vmem(1)[0],
        scratch_shapes=[dma(sp), dma(sp), pair, pair, pair, pair, dma(1)],
        compiler_params=params(number),
    )(x)


def collect_kernel(
    sp, tp, x, out, first, joined, second, total, csend, crecv, fsend, frecv, asend, arecv, local
):
    me = lax.axis_index("sp")
    j, chip, core, chips, partner = tp_places(tp)
    others = [lax.rem(chip + d, chips) * 2 + core for d in range(1, chips)]
    greet(
        [{"sp": lax.rem(me + d, sp)} for d in range(1, sp)]
        + [{"tp": o} for o in others]
        + [{"tp": partner}]
    )

    def rows(d):
        return lax.rem(me + d, sp)

    def aim(k):
        return lax.rem(chip + k, chips)

    def beside(d, k):
        s = rows(d)
        return remote(
            x.at[aim(k) * 2 + (1 - core), s],
            first.at[k, s],
            csend.at[d, k],
            crecv.at[d, k],
            {"tp": partner},
        )

    def over(d, k):
        s = rows(d)
        return remote(
            joined.at[k, s], second.at[k, s], fsend.at[d, k], frecv.at[d, k], {"tp": others[k - 1]}
        )

    def back(d):
        s = rows(d)
        return remote(total.at[s], out.at[me], asend.at[d], arecv.at[d], {"sp": s})

    def begin(i):
        d = lax.rem(i + 1, sp)
        for k in range(chips):
            beside(d, lax.rem(k + 1, chips)).start()

    each(sp, begin)

    def join(d):
        s = rows(d)
        for k in range(1, chips):
            beside(d, k).wait_recv()
            mine = x[aim(k) * 2 + core, s].astype(jnp.float32)
            joined[k, s] = (mine + first[k, s].astype(jnp.float32)).astype(joined.dtype)
            over(d, k).start()

    def close(d):
        s = rows(d)
        beside(d, 0).wait_recv()
        value = x[j, s].astype(jnp.float32) + first[0, s].astype(jnp.float32)
        for k in range(1, chips):
            over(d, k).wait_recv()
            value = value + second[k, s].astype(jnp.float32)
        total[s] = value.astype(total.dtype)

    join(lax.rem(1, sp))

    def step(i):
        join(lax.rem(i + 2, sp))
        close(i + 1)
        back(i + 1).start()

    each(sp - 1, step)
    close(0)
    own = pltpu.make_async_copy(total.at[me], out.at[me], local.at[0])
    own.start()

    def finish(d):
        for k in range(chips):
            beside(d, k).wait_send()
        for k in range(1, chips):
            over(d, k).wait_send()

    each(sp, finish)
    each(sp - 1, lambda d: back(d + 1).wait())
    own.wait()


def collect_rows(x, number):
    sp, tp = lax.axis_size("sp"), lax.axis_size("tp")
    chips = tp // 2
    pair = dma(sp, chips)
    buffer = pltpu.VMEM((chips,) + x.shape[1:], x.dtype)
    return pl.pallas_call(
        functools.partial(collect_kernel, sp, tp),
        out_shape=jax.ShapeDtypeStruct(x.shape[1:], x.dtype),
        in_specs=vmem(1),
        out_specs=vmem(1)[0],
        scratch_shapes=[
            buffer,
            buffer,
            buffer,
            pltpu.VMEM(x.shape[1:], x.dtype),
            pair,
            pair,
            pair,
            pair,
            dma(sp),
            dma(sp),
            dma(1),
        ],
        compiler_params=params(number),
    )(x)


def flip(me, d):
    out, bit = me, 1
    while bit <= d:
        if d & bit:
            out = out + bit * (1 - 2 * lax.rem(lax.div(out, bit), 2))
        bit *= 2
    return out


def expert_kernel(
    sp, tp, x, wgate, wup, wdown, out,
    arr, part, hidden, first, joined, second, total, vgate, vup, vdown,
    asend, arecv, fsend, frecv, rsend, rrecv, csend, crecv, osend, orecv, bsend, brecv, local, load,
):
    me = lax.axis_index("sp")
    j, chip, core, chips, partner = tp_places(tp)
    others = [lax.rem(chip + d, chips) * 2 + core for d in range(1, chips)]
    cap, width = x.shape[1], x.shape[2]
    ff = vgate.shape[1]
    rows = 2 * tp * cap
    loads = [
        pltpu.make_async_copy(wgate.at[0], vgate, load.at[0]),
        pltpu.make_async_copy(wup.at[0], vup, load.at[1]),
        pltpu.make_async_copy(wdown.at[0], vdown, load.at[2]),
    ]
    for copy in loads:
        copy.start()
    own = pltpu.make_async_copy(x.at[me], arr.at[me, j], local.at[0])
    own.start()
    greet(
        [{"sp": flip(me, d)} for d in range(1, sp)]
        + [{"tp": o} for o in others]
        + [{"tp": partner}]
    )

    def across(d):
        peer = flip(me, d)
        return remote(x.at[peer], arr.at[me, j], asend.at[d], arecv.at[d], {"sp": peer})

    def forward(d, k):
        spot = arr.at[flip(me, d), j]
        return remote(spot, spot, fsend.at[d, k], frecv.at[d, k], {"tp": others[k - 1]})

    def relay(d, k):
        came = lax.rem(chip + chips - k, chips) * 2 + core
        spot = arr.at[flip(me, d), came]
        return remote(spot, spot, rsend.at[d, k], rrecv.at[d, k], {"tp": partner})

    def onward(d):
        if d == 0:
            own.wait()
        else:
            across(d).wait_recv()
        for k in range(1, chips):
            forward(d, k).start()
        relay(d, 0).start()

    def pass_on(d):
        for k in range(1, chips):
            forward(d, k).wait_recv()
            relay(d, k).start()

    def aim(k):
        return lax.rem(chip + k, chips)

    def beside(d, k):
        s = flip(me, d)
        return remote(
            part.at[s, aim(k) * 2 + (1 - core)],
            first.at[s, k],
            csend.at[d, k],
            crecv.at[d, k],
            {"tp": partner},
        )

    def over(d, k):
        s = flip(me, d)
        return remote(
            joined.at[s, k], second.at[s, k], osend.at[d, k], orecv.at[d, k], {"tp": others[k - 1]}
        )

    def back(d):
        s = flip(me, d)
        return remote(total.at[s], out.at[me], bsend.at[d], brecv.at[d], {"sp": s})

    def begin(d):
        for k in range(chips):
            beside(d, (k + 1) % chips).start()

    def join(d):
        s = flip(me, d)
        for k in range(1, chips):
            beside(d, k).wait_recv()
            mine = part[s, aim(k) * 2 + core].astype(jnp.float32)
            joined[s, k] = (mine + first[s, k].astype(jnp.float32)).astype(joined.dtype)
            over(d, k).start()

    def close(d):
        s = flip(me, d)
        beside(d, 0).wait_recv()
        value = part[s, j].astype(jnp.float32) + first[s, 0].astype(jnp.float32)
        for k in range(1, chips):
            over(d, k).wait_recv()
            value = value + second[s, k].astype(jnp.float32)
        if d == 0:
            out[me] = value.astype(out.dtype)
        else:
            total[s] = value.astype(total.dtype)
            back(d).start()

    tile = min(ff, 256)
    wide = min(width, 512)

    def gate_up(g):
        base = flip(me, 2 * g) - lax.rem(flip(me, 2 * g), 2)

        def step(f):
            cols = pl.ds(pl.multiple_of(f * tile, tile), tile)
            held = arr[pl.ds(base, 2)].reshape(rows, width)
            gate = jnp.dot(held, vgate[:, cols], preferred_element_type=jnp.float32)
            up = jnp.dot(held, vup[:, cols], preferred_element_type=jnp.float32)
            hidden[:, cols] = (gate / (1.0 + jnp.exp(-gate)) * up).astype(hidden.dtype)

        each(ff // tile, step)

    def down(g):
        base = flip(me, 2 * g) - lax.rem(flip(me, 2 * g), 2)

        def step(f):
            cols = pl.ds(pl.multiple_of(f * wide, wide), wide)
            value = jnp.dot(hidden[...], vdown[:, cols], preferred_element_type=jnp.float32)
            part[pl.ds(base, 2), :, :, cols] = value.astype(part.dtype).reshape(2, tp, cap, wide)

        each(width // wide, step)

    order = [0, 1] + list(range(2, sp // 2))[::-1]
    line = [d for g in order for d in (2 * g, 2 * g + 1)]
    for d in line[1:]:
        across(d).start()
    ahead = min(4, sp)
    with jax.named_scope('prologue'):
        onward(0)
        onward(1)
        onward(2)
        pass_on(0)
        onward(3)
        pass_on(1)
    for copy in loads[:2]:
        copy.wait()
    count = len(order)
    near = line[2:4] + line[:2] if count > 2 else line[:2]

    def collect(ds):
        for d in ds:
            begin(d)
        with jax.named_scope('join'):
            for d in ds:
                join(d)

    def settle(ds):
        with jax.named_scope('close'):
            for d in ds:
                close(d)

    def carry(p):
        if p + 2 < sp:
            with jax.named_scope('onward'):
                onward(line[p + 2])
        if p < sp:
            with jax.named_scope('pass'):
                pass_on(line[p])

    sent, closed = [], 0
    for i, g in enumerate(order):
        with jax.named_scope('relayw'):
            for d in line[2 * i : 2 * i + 2]:
                for k in range(chips):
                    relay(d, k).wait_recv()
        with jax.named_scope('gateup'):
            gate_up(g)
        carry(2 * i + 2)
        settle(sent[closed : closed + 2])
        closed = min(len(sent), closed + 2)
        if i == 0:
            loads[2].wait()
        with jax.named_scope('down'):
            down(g)
        carry(2 * i + 3)
        ds = line[2 * i : 2 * i + 2]
        if i == count - 1:
            ds = ds + near if ds[0] not in near else near[2:] + ds + near[:2]
            ds = [d for d in ds if d not in sent]
        elif i >= 2:
            ds = ds + [near.pop(0)] if len(near) > 3 else ds
        elif i < 2:
            ds = []
        collect(ds)
        sent = sent + ds
    settle(sent[closed:])
    for d in range(sp):
        for k in range(1, chips):
            forward(d, k).wait_send()
            over(d, k).wait_send()
        for k in range(chips):
            relay(d, k).wait_send()
            beside(d, k).wait_send()
        if d > 0:
            across(d).wait_send()
            back(d).wait()


def run_experts(x, wgate, wup, wdown, number):
    sp, tp = lax.axis_size("sp"), lax.axis_size("tp")
    chips = tp // 2
    cap, width = x.shape[1:]
    ff = wgate.shape[2]
    kind = x.dtype
    pair = dma(sp, chips)
    line = dma(sp)
    piece = pltpu.VMEM((sp, chips, cap, width), kind)
    return pl.pallas_call(
        functools.partial(expert_kernel, sp, tp),
        out_shape=jax.ShapeDtypeStruct(x.shape, kind),
        in_specs=vmem(1) + [pl.BlockSpec(memory_space=pl.ANY)] * 3,
        out_specs=vmem(1)[0],
        scratch_shapes=[
            pltpu.VMEM((sp, tp, cap, width), kind),
            pltpu.VMEM((sp, tp, cap, width), kind),
            pltpu.VMEM((2 * tp * cap, ff), kind),
            piece,
            piece,
            piece,
            pltpu.VMEM((sp, cap, width), kind),
            pltpu.VMEM(wgate.shape[1:], kind),
            pltpu.VMEM(wup.shape[1:], kind),
            pltpu.VMEM(wdown.shape[1:], kind),
            line, line, pair, pair, pair, pair, pair, pair, pair, pair, line, line, dma(1), dma(3),
        ],
        compiler_params=pltpu.CompilerParams(
            collective_id=number, has_side_effects=True, vmem_limit_bytes=56 * 2**20
        ),
    )(x, wgate, wup, wdown)


def padded_2(cells, width):
    count, here = lax.axis_size("sp"), lax.axis_index("sp")
    came = edges(jnp.stack([cells[:width], cells[-width:]]), 1)
    before = jnp.where(here > 0, came[0], jnp.zeros_like(came[0]))
    after = jnp.where(here < count - 1, came[1], jnp.zeros_like(came[1]))
    return jnp.concatenate([before, cells, after], axis=0)


def carried_states(forward_sum, forward_final, backward_sum, backward_final):
    count = lax.axis_size("sp")
    shape = forward_final.shape
    per_head = shape[-2]
    states = jnp.stack([forward_final, backward_final]).astype(jnp.bfloat16)
    states = states.reshape(2, count, -1, shape[-1]).swapaxes(0, 1)
    totals = jnp.stack([forward_sum, backward_sum]).reshape(2, -1)
    totals = jnp.repeat(totals, per_head, axis=1).reshape(2, count, -1).swapaxes(0, 1)
    states, totals = exchange([states, totals], "sp", 2)
    factors = jnp.exp(totals)[..., None]
    parts = states.astype(jnp.float32)
    forward, backward = [], []
    held = jnp.zeros(parts.shape[2:], jnp.float32)
    for s in range(count):
        forward.append(held)
        held = factors[s, 0] * held + parts[s, 0]
    held = jnp.zeros(parts.shape[2:], jnp.float32)
    for s in reversed(range(count)):
        backward.append(held)
        held = factors[s, 1] * held + parts[s, 1]
    both = jnp.stack([jnp.stack(forward), jnp.stack(backward[::-1])], axis=1)
    (both,) = exchange([both.astype(jnp.bfloat16)], "sp", 3)
    both = both.astype(jnp.float32)
    return both[:, 0].reshape(shape), both[:, 1].reshape(shape)


def prefix_matrix(length):
    row_index = lax.broadcasted_iota(jnp.int32, (length, length), 0)
    column_index = lax.broadcasted_iota(jnp.int32, (length, length), 1)
    return (column_index <= row_index).astype(jnp.float32)


def local_chain(states, totals, reverse):

    def advance(carried, operands):
        block_state, block_total = operands
        return (jnp.exp(block_total)[..., None, None] * carried + block_state, carried)

    start_state = jnp.zeros(states.shape[1:], jnp.float32)
    return lax.scan(advance, start_state, (states, totals), reverse=reverse)


def mix_tokens(
    value_projected,
    key_projected,
    query_projected,
    output_gate_projected,
    step_projected_raw,
    head_decay_logarithm,
    position_extra_decay,
    value_filter_weight,
    key_filter_weight,
    query_filter_weight,
    head_norm_gain,
):
    tokens = value_projected.shape[0]
    value_width = value_projected.shape[1]
    key_width = key_projected.shape[1]
    head_count = step_projected_raw.shape[2]
    group_count = key_width // STATE
    per_group = head_count // group_count
    blocks = tokens // BLOCK
    joined = jnp.concatenate([value_projected, key_projected, query_projected], axis=1)
    padded = padded_2(joined, (TAPS - 1) // 2).astype(jnp.float32)
    weights = jnp.concatenate(
        [value_filter_weight, key_filter_weight, query_filter_weight], axis=1
    ).astype(jnp.float32)
    filtered = weights[0] * padded[0:tokens]
    for offset in range(1, TAPS):
        filtered = filtered + weights[offset] * padded[offset : offset + tokens]
    values = filtered[:, :value_width].astype(jnp.bfloat16)
    key_rows = jax.nn.silu(filtered[:, value_width : value_width + key_width]).astype(jnp.bfloat16)
    key_rows = key_rows.reshape(blocks, BLOCK, group_count, STATE)
    query_rows = jax.nn.silu(filtered[:, value_width + key_width :]).astype(jnp.bfloat16)
    query_rows = query_rows.reshape(blocks, BLOCK, group_count, STATE)
    positive_step_sizes = jax.nn.softplus(step_projected_raw.astype(jnp.float32))
    decay_logarithm = (
        -jnp.exp(head_decay_logarithm)[:, None, :] * positive_step_sizes
        + position_extra_decay[None]
    )
    scaled = (
        values.astype(jnp.float32).reshape(tokens, head_count, HEAD_DIM)[None]
        * positive_step_sizes[..., None]
    ).astype(jnp.bfloat16)
    scaled = scaled.reshape(2, blocks, BLOCK, group_count, per_group, HEAD_DIM)
    log_blocks = decay_logarithm.reshape(2, blocks, BLOCK, group_count, per_group)
    running = jnp.einsum("ls,dbsgh->dblgh", prefix_matrix(BLOCK), log_blocks, precision=highest)
    forward_cum = running[0]
    backward_excl = running[1] - log_blocks[1]
    forward_total = running[0][:, -1]
    backward_total = running[1][:, -1]
    scores = jnp.einsum("blgn,bsgn->blsg", query_rows, key_rows, preferred_element_type=jnp.float32)
    position = lax.broadcasted_iota(jnp.int32, (BLOCK,), 0)
    lower_mask = (position[None, :] <= position[:, None])[None, :, :, None, None]
    upper_mask = (position[None, :] >= position[:, None])[None, :, :, None, None]
    forward_gap = jnp.where(lower_mask, forward_cum[:, :, None] - forward_cum[:, None, :], -jnp.inf)
    backward_gap = jnp.where(
        upper_mask, backward_excl[:, None, :] - backward_excl[:, :, None], -jnp.inf
    )
    forward_weight = (scores[..., None] * jnp.exp(forward_gap)).astype(jnp.bfloat16)
    backward_weight = (scores[..., None] * jnp.exp(backward_gap)).astype(jnp.bfloat16)
    inner = jnp.einsum(
        "blsgh,bsghp->blghp", forward_weight, scaled[0], preferred_element_type=jnp.float32
    )
    inner = inner + jnp.einsum(
        "blsgh,bsghp->blghp", backward_weight, scaled[1], preferred_element_type=jnp.float32
    )
    key_wide = key_rows.astype(jnp.float32)[:, :, :, None, :]
    forward_keys = (jnp.exp(forward_total[:, None] - forward_cum)[..., None] * key_wide).astype(
        jnp.bfloat16
    )
    backward_keys = (jnp.exp(backward_excl)[..., None] * key_wide).astype(jnp.bfloat16)
    forward_state = jnp.einsum(
        "bsghn,bsghp->bghpn", forward_keys, scaled[0], preferred_element_type=jnp.float32
    )
    backward_state = jnp.einsum(
        "bsghn,bsghp->bghpn", backward_keys, scaled[1], preferred_element_type=jnp.float32
    )
    forward_final, forward_before = local_chain(forward_state, forward_total, False)
    backward_final, backward_before = local_chain(backward_state, backward_total, True)
    forward_sum = jnp.sum(forward_total, axis=0)
    backward_sum = jnp.sum(backward_total, axis=0)
    entering, leaving = carried_states(
        forward_sum, forward_final, backward_sum, backward_final
    )
    forward_prior = jnp.cumsum(forward_total, axis=0) - forward_total
    backward_after = backward_sum[None] - jnp.cumsum(backward_total, axis=0)
    forward_in = jnp.exp(forward_prior)[..., None, None] * entering[None] + forward_before
    backward_in = jnp.exp(backward_after)[..., None, None] * leaving[None] + backward_before
    forward_read = jnp.exp(forward_cum)[..., None] * jnp.einsum(
        "blgn,bghpn->blghp",
        query_rows,
        forward_in.astype(jnp.bfloat16),
        preferred_element_type=jnp.float32,
    )
    backward_read = jnp.exp(backward_total[:, None] - backward_excl)[..., None] * jnp.einsum(
        "blgn,bghpn->blghp",
        query_rows,
        backward_in.astype(jnp.bfloat16),
        preferred_element_type=jnp.float32,
    )
    mixer_raw = (inner + forward_read + backward_read).reshape(tokens, head_count, HEAD_DIM)
    gated = mixer_raw * jax.nn.silu(output_gate_projected.astype(jnp.float32)).reshape(
        tokens, head_count, HEAD_DIM
    )
    inverse_rms = lax.rsqrt(jnp.mean(gated * gated, axis=-1, keepdims=True) + epsilon)
    head_normed = (gated * inverse_rms * head_norm_gain.reshape(head_count, HEAD_DIM)).astype(
        jnp.bfloat16
    )
    return head_normed.reshape(tokens, head_count * HEAD_DIM)


def mixer_kernel(
    n, span, far_value, far_key, far_query, far_gate, far_raw, far_rate, far_extra,
    far_vfilter, far_kfilter, far_qfilter, far_gain, far_matrix, out,
    value, key, query, gate, raw, rate, extra, vfilter, kfilter, qfilter, gain, matrix,
    hv, hk, hq, pad, vals, keys, queries, turned, column, lines, totals, inner, weight,
    fin, met, came, gone, given, result,
    gathered, product, mine, theirs,
    esend, erecv, tsend, trecv, xsend, xrecv, zsend, zrecv, ysend, yrecv, load,
    fsend, frecv, rsend, rrecv, psend, precv,
):
    far = [far_value, far_key, far_query, far_raw, far_rate, far_extra, far_vfilter, far_kfilter,
           far_qfilter, far_gain, far_gate, far_matrix]
    near = [value, key, query, raw, rate, extra, vfilter, kfilter, qfilter, gain, gate, matrix]
    loads = [pltpu.make_async_copy(far[i], near[i], load.at[i]) for i in range(len(far))]
    for copy in loads:
        copy.start()
    me = lax.axis_index("sp")
    b, a = lax.rem(me, 2), lax.div(me, 2)
    beside, planes = me + 1 - 2 * b, n // 2
    tp = gathered.shape[0]
    j, chip, core, chips, partner = tp_places(tp)
    others = [lax.rem(chip + d, chips) * 2 + core for d in range(1, chips)]
    tokens, wide = value.shape
    heads = raw.shape[1]
    groups = key.shape[1] // STATE
    tiles = wide // LANES
    per = tiles // groups
    half = tiles // 2
    chunks = half // span
    f32 = jnp.float32

    edge = hv.shape[1]
    arrays = [(value, hv), (key, hk), (query, hq)]

    def edge_copy(i, way):
        src, halo = arrays[i]
        start, peer = (tokens - edge, lax.rem(me + 1, n)) if way == 0 else (0, lax.rem(me + n - 1, n))
        return remote(
            src.at[pl.ds(start, edge)], halo.at[way], esend.at[i, way], erecv.at[i, way], {"sp": peer}
        )

    with jax.named_scope('greet'):
        greet(
            [{"sp": lax.rem(me + d, n)} for d in range(1, n)]
            + [{"tp": lax.rem(j + d, tp)} for d in range(1, tp)]
        )
    for copy in loads[:3]:
        copy.wait()
    sends = [me < n - 1, me > 0]
    waits = [me > 0, me < n - 1]
    for way in range(2):

        @pl.when(sends[way])
        def _():
            for i in range(3):
                edge_copy(i, way).start()

        @pl.when(jnp.logical_not(waits[way]))
        def _():
            for _, halo in arrays:
                halo[way] = jnp.zeros(halo.shape[1:], halo.dtype)

    for copy in loads[3:-2]:
        copy.wait()
    row = lax.broadcasted_iota(jnp.int32, (tokens, tokens), 0)
    col = lax.broadcasted_iota(jnp.int32, (tokens, tokens), 1)
    prefix = (row <= col).astype(f32)
    lane = lax.broadcasted_iota(jnp.int32, (tokens, LANES), 1)
    lines[...] = jnp.zeros(lines.shape, f32)
    same_head = lax.broadcasted_iota(jnp.int32, (heads, heads), 0) == lax.broadcasted_iota(
        jnp.int32, (heads, heads), 1
    )

    def keep_line(q, x):
        lines[pl.ds(q * heads, heads), :] = x

    for d in range(2):
        r = raw[d].astype(f32)
        step = jnp.maximum(r, 0.0) + jnp.log1p(jnp.exp(-jnp.abs(r)))
        across_heads = jnp.broadcast_to(-jnp.exp(rate[pl.ds(d, 1), :]), (heads, heads))
        speed = jnp.sum(jnp.where(same_head, across_heads, 0.0), axis=1, keepdims=True)
        decay = speed * step + extra[...]
        total = jnp.dot(decay, prefix, preferred_element_type=f32, precision=highest)
        last = total[:, tokens - 1 : tokens]
        part = total if d == 0 else total - decay
        keep_line(d, part)
        keep_line(2 + d, step)
        keep_line(4 + d, jnp.exp(last - total if d == 0 else part) * step)
        keep_line(6 + d, jnp.exp(total if d == 0 else last - part))
    column[...] = lines[...].T
    totals[0, 0] = jnp.broadcast_to(column[tokens - 1 : tokens, :], totals.shape[2:])
    totals[0, 1] = jnp.broadcast_to(column[0:1, :], totals.shape[2:])

    def total_copy():
        return remote(totals.at[0], totals.at[1], tsend.at[0], trecv.at[0], {"sp": beside})

    total_copy().start()

    for way in range(2):

        @pl.when(waits[way])
        def _():
            for i in range(3):
                edge_copy(i, way).wait_recv()

    def convolve(src, halo, taps, store):
        reach = (TAPS - 1) // 2

        def step(i):
            cols = pl.ds(pl.multiple_of(i * LANES, LANES), LANES)
            pad[pl.ds(8, tokens)] = src[:, cols].astype(f32)
            pad[pl.ds(0, 8)] = halo[0, :, cols].astype(f32)[edge - 8 :]
            pad[pl.ds(8 + tokens, 8)] = halo[1, :, cols].astype(f32)[:8]
            w = taps[:, cols].astype(f32)
            acc = w[0:1] * pad[pl.ds(8 - reach, tokens)]
            for o in range(1, TAPS):
                acc = acc + w[o : o + 1] * pad[pl.ds(8 - reach + o, tokens)]
            store(i, cols, acc)

        each(src.shape[1] // LANES, step)

    def silu(v):
        return v / (1.0 + jnp.exp(-v))

    def keep_values(i, cols, acc):
        vals[:, cols] = acc.astype(vals.dtype)

    def keep_keys(i, cols, acc):
        acc = silu(acc)
        keys[:, cols] = acc.astype(keys.dtype)
        turned[i] = acc.T.astype(turned.dtype)

    def keep_queries(i, cols, acc):
        queries[:, cols] = silu(acc).astype(queries.dtype)

    with jax.named_scope('conv'):
        convolve(value, hv, vfilter, keep_values)
        convolve(key, hk, kfilter, keep_keys)

    def spread(x, k):
        low, high = x[:, k : k + 1], x[:, k + 1 : k + 2]
        return jnp.where(lane[: x.shape[0]] < HEAD_DIM, low, high)

    def shifted(q, first):
        return pltpu.roll(column[...], lax.rem(2 * LANES - q * heads - first, LANES), 1)

    def cross(d, c):
        spot = pl.ds((1 - b) * half + c * span, span)
        return remote(
            fin.at[d, spot], met.at[d, pl.ds(c * span, span)], xsend.at[d, c], xrecv.at[d, c], {"sp": beside}
        )

    def states(i):
        g = lax.rem(i + (1 - b) * (groups // 2), groups)
        for d in range(2):
            scale = shifted(4 + d, g * 2 * per)
            for k in range(per):
                cols = pl.ds(pl.multiple_of((g * per + k) * LANES, LANES), LANES)
                scaled = (vals[:, cols].astype(f32) * spread(scale, 2 * k)).astype(vals.dtype)
                fin[d, g * per + k] = jnp.dot(
                    turned[g], scaled, preferred_element_type=f32
                ).astype(fin.dtype)

    with jax.named_scope('states'):
        each(groups, states)
    for c in range(chunks):
        for d in range(2):
            cross(d, c).start()
    with jax.named_scope('convq'):
        convolve(query, hq, qfilter, keep_queries)

    block_row = lax.broadcasted_iota(jnp.int32, (BLOCK, BLOCK), 0)
    block_col = lax.broadcasted_iota(jnp.int32, (BLOCK, BLOCK), 1)

    def within(g):
        kcols = pl.ds(pl.multiple_of(g * STATE, STATE), STATE)
        scores = lax.dot_general(
            queries[:, kcols], keys[:, kcols], (((1,), (1,)), ((), ())), preferred_element_type=f32
        )
        first = g * 2 * per
        ahead, behind = shifted(0, first), shifted(1, first)
        for k in range(2 * per):
            fr, er = lines[pl.ds(0 * heads + first + k, 1), :], lines[pl.ds(1 * heads + first + k, 1), :]
            sf, sb = lines[pl.ds(2 * heads + first + k, 1), :], lines[pl.ds(3 * heads + first + k, 1), :]
            for i in range(tokens // BLOCK):
                rows = slice(i * BLOCK, (i + 1) * BLOCK)
                fc = jnp.broadcast_to(ahead[rows, k : k + 1], (BLOCK, BLOCK))
                ec = jnp.broadcast_to(behind[rows, k : k + 1], (BLOCK, BLOCK))
                for m in range(tokens // BLOCK):
                    cols = slice(m * BLOCK, (m + 1) * BLOCK)
                    if m < i:
                        gap, size = fc - fr[:, cols], sf[:, cols]
                    elif m > i:
                        gap, size = er[:, cols] - ec, sb[:, cols]
                    else:
                        lower, upper = block_col <= block_row, block_col >= block_row
                        gap = jnp.where(lower, fc - fr[:, cols], er[:, cols] - ec)
                        size = jnp.where(lower, sf[:, cols], 0.0) + jnp.where(upper, sb[:, cols], 0.0)
                    weight[k % 2, rows, cols] = (scores[rows, cols] * jnp.exp(gap) * size).astype(
                        weight.dtype
                    )
            if k % 2 == 1:
                spot = pl.ds(pl.multiple_of((g * per + k // 2) * LANES, LANES), LANES)
                both = vals[:, spot]
                low = jnp.dot(weight[0], both, preferred_element_type=f32)
                high = jnp.dot(weight[1], both, preferred_element_type=f32)
                inner[:, spot] = jnp.where(lane < HEAD_DIM, low, high)

    with jax.named_scope('within'):
        each(groups, within)

    with jax.named_scope('totw'):
        total_copy().wait()
    early = b == 0
    count = 2 * half

    def chain(d, c):
        peer = lax.rem(me + n + 2 - 4 * d, n)
        spot = pl.ds(c * span, span)
        return remote(gone.at[d, spot], came.at[d, spot], zsend.at[d, c], zrecv.at[d, c], {"sp": peer})

    def answer(d, c, side):
        there = pl.ds(side * half + c * span, span)
        return remote(
            given.at[d, pl.ds(c * span, span)], result.at[d, there], ysend.at[d, c], yrecv.at[d, c], {"sp": beside}
        )

    def link(d, c):
        with jax.named_scope('crossw'):
            cross(d, c).wait_recv()
        starts = a == d * (planes - 1)
        ends = a == (1 - d) * (planes - 1)

        @pl.when(starts)
        def _():
            came[d, pl.ds(c * span, span)] = jnp.zeros((span,) + came.shape[2:], came.dtype)

        @pl.when(jnp.logical_not(starts))
        def _():
            with jax.named_scope('chainw'):
                chain(d, c).wait_recv()

        near_first = b == d
        turn = lax.rem(2 * LANES - (6 + d) * heads - b * count, LANES)
        ours = pltpu.roll(totals[0, d], turn, 1)
        theirs = pltpu.roll(totals[1, d], turn, 1)
        for k in range(span):
            u = c * span + k
            mine, other = spread(ours, 2 * u)[0:1], spread(theirs, 2 * u)[0:1]
            state = came[d, u].astype(f32)
            own = fin[d, b * half + u].astype(f32)
            got = met[d, u].astype(f32)
            head = jnp.where(near_first, own, got)
            tail = jnp.where(near_first, got, own)
            head_factor = jnp.where(near_first, mine, other)
            tail_factor = jnp.where(near_first, other, mine)
            middle = head_factor * state + head
            gone[d, u] = (tail_factor * middle + tail).astype(gone.dtype)
            result[d, b * half + u] = jnp.where(near_first, state, middle).astype(result.dtype)
            given[d, u] = jnp.where(near_first, middle, state).astype(given.dtype)

        @pl.when(jnp.logical_not(ends))
        def _():
            chain(d, c).start()

        answer(d, c, b).start()

    late = jnp.where(2 * a < planes, 0, 1)
    for i in range(2):
        for c in range(chunks):
            link(late + i - 2 * late * i, c)

    block = lax.broadcasted_iota(jnp.int32, (LANES, LANES), 0) // HEAD_DIM
    share = jnp.where(
        block == lax.broadcasted_iota(jnp.int32, (LANES, LANES), 1) // HEAD_DIM, 1.0 / HEAD_DIM, 0.0
    ).astype(vals.dtype)

    def finish(u):
        g = lax.div(u, per)
        kcols = pl.ds(pl.multiple_of(g * STATE, STATE), STATE)
        cols = pl.ds(pl.multiple_of(u * LANES, LANES), LANES)
        q = queries[:, kcols]
        mixed = inner[:, cols]
        for d in range(2):
            carried = jnp.dot(q, result[d, u], preferred_element_type=f32)
            mixed = mixed + spread(shifted(6 + d, 2 * u), 0) * carried
        gated = mixed * silu(gate[:, cols].astype(f32))
        square = gated * gated
        top = square.astype(share.dtype)
        rest = (square - top.astype(f32)).astype(share.dtype)
        mean = jnp.dot(top, share, preferred_element_type=f32)
        mean = mean + jnp.dot(rest, share, preferred_element_type=f32)
        gathered[j, u] = (gated * lax.rsqrt(mean + epsilon) * gain[:, cols]).astype(gathered.dtype)

    def place(i):
        return lax.rem(b * half + i, tiles)

    def forward(i, k):
        spot = gathered.at[j, place(i)]
        return remote(spot, spot, fsend.at[i, k], frecv.at[i, k], {"tp": others[k - 1]})

    def source(k):
        return lax.rem(chip + chips - k, chips) * 2 + core

    def relay(i, k):
        spot = gathered.at[source(k), place(i)]
        return remote(spot, spot, rsend.at[i, k], rrecv.at[i, k], {"tp": partner})

    def push(i):
        for k in range(1, chips):
            forward(i, k).start()
        relay(i, 0).start()

    def stage(first):
        def step(i):
            finish(place(first + i))

            @pl.when(i > 0)
            def _():
                push(first + i - 1)

        each(half, step)
        push(first + half - 1)

    loads[-2].wait()
    with jax.named_scope('fin1'):
        stage(0)
    for c in range(chunks):
        for d in range(2):
            with jax.named_scope('answerw'):
                answer(d, c, 1 - b).wait_recv()
    with jax.named_scope('fin2'):
        stage(half)

    def multiply(src, h, start=False):
        base = place(h * half)
        left = jnp.concatenate([gathered[src, base + t] for t in range(half)], axis=1)
        depth = half * LANES
        right = matrix[pl.ds(pl.multiple_of((src * tiles + base) * LANES, LANES), depth), :]
        value = jnp.dot(left, right, preferred_element_type=f32)
        product[...] = value if start else product[...] + value

    loads[-1].wait()
    with jax.named_scope('mm0'):
        multiply(j, 0, True)
        multiply(j, 1)
    for h in range(2):
        with jax.named_scope('gatherw'):
            for i in range(h * half, (h + 1) * half):
                for k in range(1, chips):
                    forward(i, k).wait_recv()
                    relay(i, k).start()
        for i in range(h * half, (h + 1) * half):
            relay(i, 0).wait_recv()
        multiply(partner, h)
        for k in range(1, chips):
            multiply(source(k), h)
    for h in range(2):
        for k in range(1, chips):
            with jax.named_scope('relayw'):
                for i in range(h * half, (h + 1) * half):
                    relay(i, k).wait_recv()
            multiply(source(k) + 1 - 2 * core, h)
    rows = tokens // tp
    width = product.shape[1]

    def hand(d):
        peer = lax.rem(j + d, tp)
        return remote(mine.at[peer], theirs.at[j], psend.at[d], precv.at[d], {"tp": peer})

    for d in list(range(1, tp)) + [0]:
        peer = lax.rem(j + d, tp)
        block = product[pl.ds(pl.multiple_of(peer * rows, rows), rows), :].astype(mine.dtype)
        if d == 0:
            out[:, pl.ds(pl.multiple_of(j * width, LANES), width)] = block
        else:
            mine[peer] = block
    for d in range(1, tp):
        hand(d).start()
    for d in range(1, tp):
        with jax.named_scope('handw'):
            hand(d).wait_recv()
        src = lax.rem(j + tp - d, tp)
        out[:, pl.ds(pl.multiple_of(src * width, LANES), width)] = theirs[src]
    for i in range(tiles):
        for k in range(chips):
            relay(i, k).wait_send()
            if k > 0:
                forward(i, k).wait_send()
    for d in range(1, tp):
        hand(d).wait_send()

    for way in range(2):

        @pl.when(sends[way])
        def _():
            for i in range(3):
                edge_copy(i, way).wait_send()

    for c in range(chunks):
        for d in range(2):
            ends = a == planes - 1 if d == 0 else a == 0
            cross(d, c).wait_send()
            answer(d, c, b).wait_send()

            @pl.when(jnp.logical_not(ends))
            def _():
                chain(d, c).wait_send()


def run_mixer(
    value, key, query, gate, raw, rate, extra, vfilter, kfilter, qfilter, gain, matrix, number
):
    n, tp = lax.axis_size("sp"), lax.axis_size("tp")
    tokens, wide = value.shape
    rows, width = tokens // tp, matrix.shape[1]
    narrow = key.shape[1]
    groups, tiles = narrow // STATE, wide // LANES
    half = tiles // 2
    span = 2 if half % 2 == 0 else 1
    kind, f32 = value.dtype, jnp.float32
    edge = 16
    state = pltpu.VMEM((2, half, STATE, LANES), kind)
    full = pltpu.VMEM((2, tiles, STATE, LANES), kind)
    sems = dma(2, half // span)
    operands = [
        value, key, query, gate, raw.swapaxes(1, 2), rate, extra.T,
        vfilter, kfilter, qfilter, gain.reshape(1, -1), matrix,
    ]
    pairs = dma(tiles, tp // 2)
    return pl.pallas_call(
        functools.partial(mixer_kernel, n, span),
        out_shape=jax.ShapeDtypeStruct((rows, tp * width), kind),
        in_specs=[pl.BlockSpec(memory_space=pltpu.HBM)] * len(operands),
        out_specs=vmem(1)[0],
        scratch_shapes=[
            *[pltpu.VMEM(x.shape, x.dtype) for x in operands],
            pltpu.VMEM((2, edge, wide), kind),
            pltpu.VMEM((2, edge, narrow), kind),
            pltpu.VMEM((2, edge, narrow), kind),
            pltpu.VMEM((tokens + 16, LANES), f32),
            pltpu.VMEM((tokens, wide), kind),
            pltpu.VMEM((tokens, narrow), kind),
            pltpu.VMEM((tokens, narrow), kind),
            pltpu.VMEM((groups, STATE, tokens), kind),
            pltpu.VMEM((tokens, LANES), f32),
            pltpu.VMEM((LANES, tokens), f32),
            pltpu.VMEM((2, 2, 8, LANES), f32),
            pltpu.VMEM((tokens, wide), f32),
            pltpu.VMEM((2, tokens, tokens), kind),
            full, state, state, state, state, full,
            pltpu.VMEM((tp, tiles, tokens, LANES), kind),
            pltpu.VMEM((tokens, width), f32),
            pltpu.VMEM((tp, rows, width), kind),
            pltpu.VMEM((tp, rows, width), kind),
            dma(3, 2), dma(3, 2), dma(1), dma(1), sems, sems, sems, sems, sems, sems, dma(len(operands)),
            pairs, pairs, pairs, pairs, dma(tp), dma(tp),
        ],
        compiler_params=pltpu.CompilerParams(
            collective_id=number, has_side_effects=True
        ),
    )(*operands)


def slot_table(route_rows, experts, capacity):
    flat_ids = route_rows.reshape(-1)
    expert_ids = lax.broadcasted_iota(jnp.int32, (flat_ids.shape[0], experts), 1)
    matches = (flat_ids[:, None] == expert_ids).astype(jnp.int32)
    earlier = jnp.cumsum(matches, axis=0) - matches
    rank_in = jnp.sum(matches * earlier, axis=1)
    return (flat_ids * capacity + rank_in).reshape(route_rows.shape)


def dispatch_rows(slots, token_rows, places):
    place_ids = lax.broadcasted_iota(jnp.int32, (places,) + slots.shape, 0)
    one_hot = jnp.sum((place_ids == slots[None]).astype(jnp.float32), axis=2).astype(jnp.bfloat16)
    return jnp.dot(one_hot, token_rows, preferred_element_type=jnp.float32).astype(jnp.bfloat16)


def shards(
    residual_layer_input,
    value_projected,
    key_projected,
    query_projected,
    output_gate_projected,
    step_projected_raw,
    head_decay_logarithm,
    position_extra_decay,
    value_filter_weight,
    key_filter_weight,
    query_filter_weight,
    head_norm_gain,
    mixer_output_matrix,
    expert_norm_gain,
    routes,
    chosen_expert_weight,
    expert_gate_matrix,
    expert_up_matrix,
    expert_down_matrix,
):
    operands = (
        value_projected,
        key_projected,
        query_projected,
        output_gate_projected,
        step_projected_raw,
        head_decay_logarithm,
        position_extra_decay,
        value_filter_weight,
        key_filter_weight,
        query_filter_weight,
        head_norm_gain,
    )
    if value_projected.shape[1] % (2 * LANES) == 0 and 8 * step_projected_raw.shape[2] <= LANES and lax.axis_size("sp") % 2 == 0:
        mixer_out = run_mixer(*operands, mixer_output_matrix, 2)
    else:
        projected = jnp.dot(
            gather_columns(mix_tokens(*operands), 4),
            mixer_output_matrix,
            preferred_element_type=jnp.float32,
        ).astype(jnp.bfloat16)
        tp = lax.axis_size("tp")
        (columns,) = exchange([projected.reshape(tp, -1, projected.shape[1])], "tp", 5)
        mixer_out = columns.swapaxes(0, 1).reshape(columns.shape[1], -1)
    middle = (residual_layer_input.astype(jnp.float32) + mixer_out.astype(jnp.float32)).astype(
        jnp.bfloat16
    )
    residual = middle.astype(jnp.float32)
    normed = (
        residual
        * lax.rsqrt(jnp.mean(residual * residual, axis=-1, keepdims=True) + epsilon)
        * expert_norm_gain
    ).astype(jnp.bfloat16)
    own_rows = normed.shape[0]
    model_width = normed.shape[1]
    top_count = routes.shape[1]
    experts = lax.axis_size("sp")
    capacity = 2 * own_rows * top_count // experts
    places = experts * capacity
    position = lax.axis_index("tp")
    own_routes = lax.dynamic_slice_in_dim(routes, position * own_rows, own_rows, 0)
    own_slots = slot_table(own_routes, experts, capacity)
    outgoing = dispatch_rows(own_slots, normed, places)
    slotted = outgoing.reshape(experts, capacity, model_width)
    if capacity % 16 == 0 and experts & (experts - 1) == 0 and experts >= 4:
        returned = run_experts(
            slotted, expert_gate_matrix, expert_up_matrix, expert_down_matrix, 6
        )
    else:
        arrived = spread_rows(slotted, 6)
        slot_rows = arrived.reshape(-1, model_width)
        gate_value = jnp.dot(slot_rows, expert_gate_matrix[0], preferred_element_type=jnp.float32)
        up_value = jnp.dot(slot_rows, expert_up_matrix[0], preferred_element_type=jnp.float32)
        hidden = (jax.nn.silu(gate_value) * up_value).astype(jnp.bfloat16)
        partial_sum = jnp.dot(hidden, expert_down_matrix[0], preferred_element_type=jnp.float32).astype(
            jnp.bfloat16
        )
        returned = collect_rows(partial_sum.reshape(arrived.shape), 7)
    chosen = (
        lax.broadcasted_iota(jnp.int32, (own_rows, top_count, places), 2) == own_slots[:, :, None]
    )
    mixing = jnp.sum(jnp.where(chosen, chosen_expert_weight[:, :, None], 0.0), axis=1)
    expert_mix = jnp.dot(
        mixing, returned.reshape(places, model_width).astype(jnp.float32), precision=highest
    )
    return (residual + expert_mix).astype(jnp.bfloat16)


def solution(mesh):
    return jax.shard_map(
        shards,
        mesh=mesh,
        in_specs=(
            P(("sp", "tp"), None),
            P("sp", "tp"),
            P("sp", "tp"),
            P("sp", "tp"),
            P("sp", "tp"),
            P(None, "sp", "tp"),
            P(None, "tp"),
            P("sp", "tp"),
            P(None, "tp"),
            P(None, "tp"),
            P(None, "tp"),
            P("tp"),
            P(None, "tp"),
            P(),
            P("sp", None),
            P(("sp", "tp"), None),
            P("sp", None, "tp"),
            P("sp", None, "tp"),
            P("sp", "tp", None),
        ),
        out_specs=P(("sp", "tp"), None),
        check_vma=False,
    )
```
